256 devices in a mesh: kv: 64 (over z, y, core), tp: 4 (over x).
Axes of the slice: x: 4, y: 4, z: 8, core: 2. Of those that a mesh axis runs over, the one named last changes fastest.
Arguments:
- inputs: bfloat16 [2048, 4096], P(None, 'kv'), may hold values from -150 to 150
- norm_gain: bfloat16 [4096], P('kv'), may hold values from 0.099609375 to 1.8984375
- w_query: bfloat16 [4096, 2048], P('kv', 'tp'), may hold values from -0.09375 to 0.09375
- w_forget: bfloat16 [4096, 2048], P('kv', 'tp'), may hold values from -0.09375 to 0.09375
- w_value: bfloat16 [4096, 2048], P('kv', 'tp'), may hold values from -0.09375 to 0.09375
- lower_bound: float32 [2048], P('tp'), may hold values from 0.05 to 0.9
- head_gain: float32 [2048], P('tp'), may hold values from 0.1 to 1.9
- w_out: bfloat16 [2048, 4096], P('tp', 'kv'), may hold values from -0.125 to 0.125
- prior_state: float32 [512, 16, 128, 128], P('kv', 'tp'), may hold values from -3 to 3
- prev_forget: float32 [512, 4, 2048], P('kv', None, 'tp'), may hold values from 0.3 to 0.97
- prev_values: bfloat16 [512, 4, 2048], P('kv', None, 'tp'), may hold values from -6 to 6
- accepted: int32 [512], P('kv'), may hold values from 0 to 4
Outputs:
- mixed_out: bfloat16 [2048, 4096], P(None, ('kv', 'tp'))
- base_state: float32 [512, 16, 128, 128], P('kv', 'tp')
The draws below stay inside these ranges and needn't reach their ends.
All inputs are finite; a program needn't handle non-finite values.
Results may differ from the reference program's by a relative error of at most 0.01.
Values may be sent and summed in bfloat16 or wider, within the bound.
A program may use at most 64 MiB of HBM per device.

```python
import jax
import jax.numpy as jnp
from jax import lax

D = 4096
HEADS = 16
HEAD_SIZE = 128
PROPOSALS = 4
HEAD_WIDTH = 2048
SEQS = 512
TOKENS = 2048
N_TP = 4


def draw_inputs(key, part):
    split_keys = jax.random.split(key, 4)
    column = jnp.arange(D, dtype=jnp.float32)[None, :] / D
    row_scale = 10.0 ** jax.random.uniform(split_keys[0], (TOKENS, 1), jnp.float32) / 3.0
    entries = jnp.clip(jax.random.normal(split_keys[1], (TOKENS, D), jnp.float32), -4.0, 4.0)
    column_scale = 10.0 ** (1.6 * column + 0.2 * jax.random.uniform(split_keys[3], (1, D), jnp.float32) - 0.9)
    return (entries * row_scale * column_scale).astype(jnp.bfloat16)


def set_ends(drawn, stream_key, smallest, largest):
    spot = [jax.random.randint(jax.random.fold_in(stream_key, axis), (), 0, length) for axis, length in enumerate(drawn.shape)]
    widest = drawn.shape.index(max(drawn.shape))
    beside = spot[:widest] + [(spot[widest] + 1) % drawn.shape[widest]] + spot[widest + 1:]
    return drawn.at[tuple(spot)].set(smallest).at[tuple(beside)].set(largest)


def shard_levels(rng, extent, pieces, low, high):
    factor_of = 1.0
    for dim, shards_of in pieces:
        draws = jax.random.uniform(jax.random.fold_in(jax.random.fold_in(rng, 6), dim), (shards_of,), jnp.float32, low / len(pieces), high / len(pieces))
        factor_of = factor_of * jnp.repeat(jnp.exp(draws), extent[dim] // shards_of).reshape((-1,) + (1,) * (len(extent) - 1 - dim))
    return factor_of


def normal_values(rng, extent, scale, reach, cuts=(), kind=jnp.bfloat16):
    result = scale * jax.random.normal(rng, extent, jnp.float32)
    if cuts:
        result = result * shard_levels(rng, extent, cuts, -0.22, 0.18)
    return jnp.clip(result, -reach, reach).astype(kind)


def setup_inputs(seed: int = 0) -> dict:
    seeds = jax.random.split(jax.random.key(seed), 13)
    return {
        "inputs": draw_inputs(jax.random.fold_in(seeds[12], 71), 0),
        "norm_gain": jnp.clip(1.0 + 0.18 * jax.random.normal(seeds[1], (D,), jnp.float32), 0.099609375, 1.8984375).astype(jnp.bfloat16),
        "w_query": normal_values(seeds[2], (D, HEAD_WIDTH), D ** -0.5, 0.09375, ((0, 64), (1, 4))),
        "w_forget": normal_values(seeds[3], (D, HEAD_WIDTH), D ** -0.5, 0.09375, ((0, 64), (1, 4))),
        "w_value": normal_values(seeds[4], (D, HEAD_WIDTH), D ** -0.5, 0.09375, ((0, 64), (1, 4))),
        "lower_bound": jnp.clip(0.05 + 0.84999998 * jax.random.uniform(seeds[5], (HEAD_WIDTH,), jnp.float32) ** shard_levels(seeds[5], (HEAD_WIDTH,), ((0, 4),), -0.2, 0.2), 0.05, 0.9),
        "head_gain": jnp.clip(1.0 + 0.18 * jax.random.normal(seeds[6], (HEAD_WIDTH,), jnp.float32), 0.1, 1.9),
        "w_out": normal_values(seeds[7], (HEAD_WIDTH, D), HEAD_WIDTH ** -0.5, 0.125, ((0, 4), (1, 64))),
        "prior_state": normal_values(seeds[8], (SEQS, HEADS, HEAD_SIZE, HEAD_SIZE), 0.5, 3.0, ((0, 64), (1, 4)), jnp.float32),
        "prev_forget": jnp.clip(0.3 + 0.67 * jax.random.uniform(seeds[9], (SEQS, PROPOSALS, HEAD_WIDTH), jnp.float32) ** shard_levels(seeds[9], (SEQS, PROPOSALS, HEAD_WIDTH), ((0, 64), (2, 4)), -0.2, 0.2), 0.3, 0.97),
        "prev_values": normal_values(seeds[10], (SEQS, PROPOSALS, HEAD_WIDTH), 1.0, 6.0, ((0, 64), (2, 4))),
        "accepted": set_ends(jax.random.randint(seeds[11], (SEQS,), 0, PROPOSALS + 1), jax.random.fold_in(seeds[11], 1), 0, PROPOSALS).astype(jnp.int32),
    }


EPSILON = 1e-06

def recurrence(query_pre, forget_pre, value_pre, lower_bound, head_gain, prior_state, prev_forget, prev_values, accepted):
    sequences = prior_state.shape[0]
    heads = prior_state.shape[1]
    head_size = prior_state.shape[2]
    proposals = prev_forget.shape[1]
    layout = (sequences, proposals, heads, head_size)
    floor_gate = lower_bound.reshape(heads, head_size)
    forget_gate = floor_gate + (1.0 - floor_gate) * jax.nn.sigmoid(forget_pre.reshape(layout))
    keys_new = 1.0 - forget_gate
    queries = jax.nn.silu(query_pre.reshape(layout))
    values = value_pre.reshape(layout)
    old_gate = prev_forget.reshape(layout)
    old_values = prev_values.astype(jnp.float32).reshape(layout)
    carried = prior_state
    for position in range(proposals):
        folded = old_gate[:, position, :, :, None] * carried + (1.0 - old_gate[:, position])[..., None] * old_values[:, position, :, None, :]
        taken_up = (position < accepted)[:, None, None, None]
        carried = jnp.where(taken_up, folded, carried)
    base_state = carried
    results = []
    for position in range(proposals):
        carried = forget_gate[:, position, :, :, None] * carried + keys_new[:, position, :, :, None] * values[:, position, :, None, :]
        results.append(jnp.einsum('shk,shkv->shv', queries[:, position], carried, precision=lax.Precision.HIGHEST))
    stacked = jnp.stack(results, axis=1)
    inverse_rms = lax.rsqrt(lax.optimization_barrier(jnp.mean(stacked * stacked, axis=-1, keepdims=True)) + EPSILON)
    normed = stacked * inverse_rms * head_gain.reshape(heads, head_size)
    return (normed.astype(jnp.bfloat16).reshape(sequences * proposals, heads * head_size), base_state)

def project(scaled, weight, rscale):
    return jnp.dot(scaled, weight, preferred_element_type=jnp.float32) * rscale[:, None]

def reference(inputs, norm_gain, w_query, w_forget, w_value, lower_bound, head_gain, w_out, prior_state, prev_forget, prev_values, accepted):
    widened = inputs.astype(jnp.float32)
    squares = lax.optimization_barrier(jnp.sum(widened * widened, axis=1))
    rscale = lax.rsqrt(squares / D + EPSILON)
    scaled = (widened * norm_gain.astype(jnp.float32)).astype(jnp.bfloat16)
    query_pre = project(scaled, w_query, rscale)
    forget_pre = project(scaled, w_forget, rscale)
    value_pre = project(scaled, w_value, rscale)
    normed, base_state = recurrence(query_pre, forget_pre, value_pre, lower_bound, head_gain, prior_state, prev_forget, prev_values, accepted)
    span_width = HEAD_WIDTH // N_TP
    mixed_out = jnp.zeros((TOKENS, D), jnp.float32)
    for member in range(N_TP):
        partial_value = jnp.dot(normed[:, member * span_width:(member + 1) * span_width], w_out[member * span_width:(member + 1) * span_width], preferred_element_type=jnp.float32)
        rounded = lax.optimization_barrier(partial_value.astype(jnp.bfloat16))
        mixed_out = mixed_out + rounded.astype(jnp.float32)
    return (mixed_out.astype(jnp.bfloat16), base_state)
```

```python
import functools

import jax
import jax.numpy as jnp
from jax import lax
from jax.experimental import pallas as pl
from jax.experimental.pallas import tpu as pltpu
from jax.sharding import Mesh
from jax.sharding import PartitionSpec as P

KV = ("kv_0", "kv_1", "kv_2")
KV_TP = ("kv_0", "kv_1", "kv_2", "tp")
MESH_ID = pl.DeviceIdType.MESH
EPSILON = 1e-06
F32 = jnp.float32
BF16 = jnp.bfloat16

D = 4096
Z, Y, C, X = 8, 4, 2, 4
G = Y * C
FEATS = 64
OWN = 32
SET = Z * OWN
TOKENS = 2048
HEADS = 4
HEAD = 128
COLS = HEADS * HEAD
SEQS = 8
STEPS = 4
CHUNKS = 3
UP, DOWN = 0, 1
HOPS = ((4, 3), (3, 4), (4, 3))


def kernel(
    x_hbm,
    gain_ref,
    wq_hbm,
    wf_hbm,
    wv_hbm,
    wo_hbm,
    floor_ref,
    head_gain_ref,
    prior_hbm,
    prev_gate_ref,
    prev_value_ref,
    accepted_ref,
    out_ref,
    base_hbm,
    x_raw,
    x_send,
    x_all,
    sq_send,
    sq_all,
    sq_mine,
    sq_z,
    w_all,
    state,
    base_low,
    part,
    ring_send,
    ring_recv,
    normed_all,
    cross_send,
    cross_recv,
    final_send,
    final_recv,
    local_sem,
    x_sems,
    sq_sems,
    sqz_sems,
    w_sems,
    ring_sems,
    normed_sems,
    cross_sems,
    final_sems,
):
    z = lax.axis_index("kv_0")
    y = lax.axis_index("kv_1")
    c = lax.axis_index("kv_2")
    x = lax.axis_index("tp")
    g = y * C + c

    def at_z(step):
        return lax.rem(z + (step + Z), Z)

    def at_y(step):
        return lax.rem(y + (step + Y), Y)

    def at_x(step):
        return lax.rem(x + (step + X), X)

    sib = 1 - c
    above, below = at_y(1), at_y(-1)
    group_steps = [(dy, dc) for dy in range(Y) for dc in range(C) if dy or dc]

    def group_peer(dy, dc):
        return at_y(dy), (sib if dc else c)

    x_load = pltpu.make_async_copy(x_hbm, x_raw, local_sem.at[0])
    x_load.start()
    w_loads = []
    for j, src in enumerate((wq_hbm, wf_hbm, wv_hbm, wo_hbm)):
        load = pltpu.make_async_copy(src, w_all.at[j, g], local_sem.at[1 + j])
        load.start()
        w_loads.append(load)
    prior_load = pltpu.make_async_copy(prior_hbm, state, local_sem.at[5])
    prior_load.start()

    barrier = pltpu.get_barrier_semaphore()
    peers = []
    for dy, dc in group_steps:
        py, pc = group_peer(dy, dc)
        peers.append((z, py, pc, x))
    for dz in range(1, Z):
        peers.append((at_z(dz), y, c, x))
    for dx in range(1, X):
        peers.append((z, y, c, at_x(dx)))
    for peer in peers:
        pl.semaphore_signal(barrier, inc=1, device_id=peer, device_id_type=MESH_ID)

    gain_col = jnp.transpose(jnp.broadcast_to(gain_ref[...].astype(F32), (HEAD, FEATS)))
    lane_block = lax.broadcasted_iota(jnp.int32, (FEATS, HEAD), 1) // OWN
    x_load.wait()
    for peer in range(G):
        for half in range(2):
            tile = None
            for k in range(4):
                zz = half * 4 + k
                src = x_raw[:, pl.ds(zz * 256 + (peer // 4) * 128, 128)].astype(F32)
                shift = ((k - peer % 4) * OWN) % 128
                if shift:
                    src = pltpu.roll(src, shift, 1)
                tile = src if tile is None else jnp.where(lane_block == k, src, tile)
            lanes = pl.ds(half * 128, 128)
            sq_send[peer, :, lanes] = jnp.sum(tile * tile, axis=0, keepdims=True)
            x_send[peer, :, lanes] = (tile * gain_col).astype(BF16)

    pl.semaphore_wait(barrier, len(peers))

    def remote(src, dst, sems, index, peer):
        return pltpu.make_async_remote_copy(
            src_ref=src,
            dst_ref=dst,
            send_sem=sems.at[0, index],
            recv_sem=sems.at[1, index],
            device_id=peer,
            device_id_type=MESH_ID,
        )

    started = []

    def go(copy):
        copy.start()
        started.append(copy)
        return copy

    x_copies, sq_copies = [], []
    for i, (dy, dc) in enumerate(group_steps):
        py, pc = group_peer(dy, dc)
        pg = py * C + pc
        peer = (z, py, pc, x)
        x_copies.append(go(remote(x_send.at[pg], x_all.at[g], x_sems, i, peer)))
        sq_copies.append(go(remote(sq_send.at[pg], sq_all.at[g], sq_sems, i, peer)))
    x_all[g] = x_send[g]
    sq_all[g] = sq_send[g]

    W = []
    for j in range(4):
        w_loads[j].wait()
        own = w_all.at[j, g]
        W.append(
            {
                "up": go(remote(own, own, w_sems, j * 8 + 0, (z, above, c, x))),
                "down": go(remote(own, own, w_sems, j * 8 + 1, (z, below, c, x))),
                "sib0": go(remote(own, own, w_sems, j * 8 + 2, (z, y, sib, x))),
            }
        )
    half = FEATS // 2
    g_below, g_above, g_far = below * C + c, above * C + c, at_y(2) * C + c

    def forward(j):
        W[j]["up"].wait_recv()
        piece = w_all.at[j, g_below, pl.ds(0, half)]
        W[j]["up2"] = go(remote(piece, piece, w_sems, j * 8 + 3, (z, above, c, x)))
        block = w_all.at[j, g_below]
        W[j]["sib1"] = go(remote(block, block, w_sems, j * 8 + 4, (z, y, sib, x)))
        W[j]["down"].wait_recv()
        piece = w_all.at[j, g_above, pl.ds(half, half)]
        W[j]["down2"] = go(remote(piece, piece, w_sems, j * 8 + 5, (z, below, c, x)))
        block = w_all.at[j, g_above]
        W[j]["sib2"] = go(remote(block, block, w_sems, j * 8 + 6, (z, y, sib, x)))

    def forward_far(j):
        W[j]["up2"].wait_recv()
        W[j]["down2"].wait_recv()
        block = w_all.at[j, g_far]
        W[j]["sib3"] = go(remote(block, block, w_sems, j * 8 + 7, (z, y, sib, x)))

    def complete(j):
        for k in range(4):
            W[j]["sib%d" % k].wait_recv()

    prior_load.wait()
    position = lax.broadcasted_iota(jnp.int32, (STEPS, COLS), 0)
    decays, keys_old, values_old = [], [], []
    for s in range(SEQS):
        taken = position < accepted_ref[s]
        gate = jnp.where(taken, prev_gate_ref[s], 1.0)
        key = 1.0 - gate
        after = jnp.ones((1, COLS), F32)
        rows = [None] * STEPS
        for j in reversed(range(STEPS)):
            rows[j] = key[j : j + 1] * after
            after = after * gate[j : j + 1]
        decays.append(after)
        keys_old.append(jnp.concatenate(rows, axis=0))
        values_old.append(prev_value_ref[s].astype(F32))
    for h in range(HEADS):
        cols = slice(h * HEAD, (h + 1) * HEAD)
        decay_cols = jnp.transpose(
            jnp.concatenate([decays[s][:, cols] for s in range(SEQS)], axis=0)
        )
        for s in range(SEQS):
            added = lax.dot_general(
                keys_old[s][:, cols],
                values_old[s][:, cols],
                (((0,), (0,)), ((), ())),
                precision=lax.Precision.HIGHEST,
                preferred_element_type=F32,
            )
            new = state[s, h] * decay_cols[:, s : s + 1] + added
            state[s, h] = new
            base_low[s, h] = new.astype(BF16)
    base_store = pltpu.make_async_copy(state, base_hbm, local_sem.at[6])
    base_store.start()

    def squares_out():
        for copy in sq_copies:
            copy.wait_recv()
        total = sq_all[0]
        for k in range(1, G):
            total = total + sq_all[k]
        sq_mine[...] = total
        copies = []
        for dz in range(1, Z):
            peer = (at_z(dz), y, c, x)
            copies.append(go(remote(sq_mine, sq_z.at[z], sqz_sems, dz - 1, peer)))
        sq_z[z] = total
        return copies

    lefts = {}

    def multiply(j):
        if "x" not in lefts:
            for copy in x_copies:
                copy.wait_recv()
            lefts["x"] = jnp.transpose(x_all[...].reshape(G * FEATS, SET))
        product = jnp.dot(
            lefts["x"], w_all[j].reshape(G * FEATS, COLS), preferred_element_type=F32
        )
        part[j] = product.reshape(Z, OWN, COLS)

    ring = {}

    def ring_step(j, step):
        for way in (UP, DOWN):
            hops = HOPS[j][way]
            if step > hops:
                continue
            sign = 1 if way == UP else -1
            value = part[j, at_z(sign * (hops - step + 1))]
            if step > 1:
                ring[j, way, step - 1].wait_recv()
                value = value + ring_recv[j, way, step - 2].astype(F32)
            ring_send[j, way, step - 1] = value.astype(BF16)
            ring[j, way, step] = go(
                remote(
                    ring_send.at[j, way, step - 1],
                    ring_recv.at[j, way, step - 1],
                    ring_sems,
                    (j * 2 + way) * 4 + step - 1,
                    (at_z(sign), y, c, x),
                )
            )

    def ring_end(j):
        value = part[j, z]
        for way in (UP, DOWN):
            ring[j, way, HOPS[j][way]].wait_recv()
            value = value + ring_recv[j, way, HOPS[j][way] - 1].astype(F32)
        return value

    forward(0)
    forward(1)
    forward_far(0)
    sqz_copies = squares_out()
    complete(0)
    multiply(0)
    ring_step(0, 1)
    forward(2)
    forward_far(1)
    complete(1)
    multiply(1)
    ring_step(1, 1)
    forward(3)
    ring_step(0, 2)
    forward_far(2)
    complete(2)
    multiply(2)
    ring_step(2, 1)
    ring_step(1, 2)
    ring_step(0, 3)
    forward_far(3)
    ring_step(2, 2)
    ring_step(1, 3)
    ring_step(0, 4)
    ring_step(2, 3)
    ring_step(1, 4)
    ring_step(2, 4)
    complete(3)

    for copy in sqz_copies:
        copy.wait_recv()
    squares = sq_z[0]
    for k in range(1, Z):
        squares = squares + sq_z[k]
    token = lax.broadcasted_iota(jnp.int32, (OWN, SET), 0) + z * OWN
    lane = lax.broadcasted_iota(jnp.int32, (OWN, SET), 1)
    own_squares = jnp.sum(
        jnp.where(lane == token, jnp.broadcast_to(squares, (OWN, SET)), 0.0),
        axis=1,
        keepdims=True,
    )
    rscale = lax.rsqrt(own_squares / D + EPSILON)

    query_pre = ring_end(0) * rscale
    forget_pre = ring_end(1) * rscale
    value_pre = ring_end(2) * rscale

    row = lax.broadcasted_iota(jnp.int32, (OWN, HEAD), 0)
    when = lax.rem(row, STEPS)
    first_seq = lax.broadcasted_iota(jnp.int32, (8, HEAD), 0) < STEPS
    for h in range(HEADS):
        cols = slice(h * HEAD, (h + 1) * HEAD)
        floor = floor_ref[h : h + 1, :]
        gate = floor + (1.0 - floor) * jax.nn.sigmoid(forget_pre[:, cols])
        key = 1.0 - gate
        pre = query_pre[:, cols]
        query = pre * jax.nn.sigmoid(pre)
        value = value_pre[:, cols]
        decayed = query
        result = jnp.sum(query * key, axis=1, keepdims=True) * value
        for back in range(1, STEPS):
            gate_back = gate if back == 1 else pltpu.roll(gate, back - 1, 0)
            decayed = decayed * (
                gate_back if back == 1 else jnp.where(when >= back - 1, gate_back, 1.0)
            )
            weight = jnp.sum(
                jnp.where(when >= back, decayed * pltpu.roll(key, back, 0), 0.0),
                axis=1,
                keepdims=True,
            )
            result = result + weight * pltpu.roll(value, back, 0)
        decayed = decayed * jnp.where(when >= STEPS - 1, pltpu.roll(gate, STEPS - 1, 0), 1.0)
        low = decayed.astype(BF16)
        carried = []
        for pair in range(SEQS // 2):
            rows = low[pair * 8 : pair * 8 + 8]
            one = jnp.dot(rows, base_low[2 * pair, h], preferred_element_type=F32)
            two = jnp.dot(rows, base_low[2 * pair + 1, h], preferred_element_type=F32)
            carried.append(jnp.where(first_seq, one, two))
        result = result + jnp.concatenate(carried, axis=0)
        mean = jnp.sum(result * result, axis=1, keepdims=True) / HEAD
        normed = result * lax.rsqrt(mean + EPSILON) * head_gain_ref[h : h + 1, :]
        normed_all[z, :, cols] = normed.astype(BF16)

    copies = []
    for i, dz in enumerate((4, 3, 5, 2, 6, 1, 7)):
        slot = normed_all.at[z]
        copies.append(go(remote(slot, slot, normed_sems, i, (at_z(dz), y, c, x))))
    for copy in copies:
        copy.wait_recv()

    product = lax.dot_general(
        w_all[3].reshape(G * FEATS, COLS),
        normed_all[...].reshape(SET, COLS),
        (((1,), (1,)), ((), ())),
        preferred_element_type=F32,
    )
    pieces = product.astype(BF16).reshape(G, X, FEATS // X, SET)
    for k in range(X):
        cross_send[k] = pieces[:, k]
    copies = []
    for dx in (2, 1, 3):
        to = at_x(dx)
        copies.append(
            go(remote(cross_send.at[to], cross_recv.at[dx - 1], cross_sems, dx - 1, (z, y, c, to)))
        )
    total = cross_send[x].astype(F32)
    for dx, copy in zip((2, 1, 3), copies):
        copy.wait_recv()
        total = total + cross_recv[dx - 1].astype(F32)
    final_send[...] = total.astype(BF16)
    copies = []
    for i, (dy, dc) in enumerate(group_steps):
        py, pc = group_peer(dy, dc)
        pg = py * C + pc
        peer = (z, py, pc, x)
        copies.append(go(remote(final_send.at[pg], final_recv.at[g], final_sems, i, peer)))
    final_recv[g] = final_send[g]
    for copy in copies:
        copy.wait_recv()

    rows_out = FEATS // X
    lane_block = lax.broadcasted_iota(jnp.int32, (rows_out, HEAD), 1) // OWN
    for zz in range(Z):
        for half_g in range(2):
            tile = None
            for k in range(4):
                src = final_recv[half_g * 4 + k, :, pl.ds((zz // 4) * 128, 128)].astype(F32)
                shift = ((k - zz % 4) * OWN) % 128
                if shift:
                    src = pltpu.roll(src, shift, 1)
                tile = src if tile is None else jnp.where(lane_block == k, src, tile)
            out_ref[:, pl.ds(zz * 256 + half_g * 128, 128)] = tile.astype(BF16)

    for copy in started:
        copy.wait_send()
    base_store.wait()


def fused(*args):
    any_space = pl.BlockSpec(memory_space=pl.ANY)
    vmem = pl.BlockSpec(memory_space=pltpu.VMEM)
    smem = pl.BlockSpec(memory_space=pltpu.SMEM)
    dma = lambda n: pltpu.SemaphoreType.DMA((2, n))
    return pl.pallas_call(
        kernel,
        out_shape=(
            jax.ShapeDtypeStruct((FEATS // X, TOKENS), BF16),
            jax.ShapeDtypeStruct((SEQS, HEADS, HEAD, HEAD), F32),
        ),
        in_specs=[any_space, vmem] + [any_space] * 4 + [vmem, vmem, any_space, vmem, vmem, smem],
        out_specs=(vmem, any_space),
        scratch_shapes=[
            pltpu.VMEM((FEATS, TOKENS), BF16),
            pltpu.VMEM((G, FEATS, SET), BF16),
            pltpu.VMEM((G, FEATS, SET), BF16),
            pltpu.VMEM((G, 1, SET), F32),
            pltpu.VMEM((G, 1, SET), F32),
            pltpu.VMEM((1, SET), F32),
            pltpu.VMEM((Z, 1, SET), F32),
            pltpu.VMEM((4, G, FEATS, COLS), BF16),
            pltpu.VMEM((SEQS, HEADS, HEAD, HEAD), F32),
            pltpu.VMEM((SEQS, HEADS, HEAD, HEAD), BF16),
            pltpu.VMEM((CHUNKS, Z, OWN, COLS), F32),
            pltpu.VMEM((CHUNKS, 2, 4, OWN, COLS), BF16),
            pltpu.VMEM((CHUNKS, 2, 4, OWN, COLS), BF16),
            pltpu.VMEM((Z, OWN, COLS), BF16),
            pltpu.VMEM((X, G, FEATS // X, SET), BF16),
            pltpu.VMEM((X - 1, G, FEATS // X, SET), BF16),
            pltpu.VMEM((G, FEATS // X, SET), BF16),
            pltpu.VMEM((G, FEATS // X, SET), BF16),
            pltpu.SemaphoreType.DMA((7,)),
            dma(G - 1),
            dma(G - 1),
            dma(Z - 1),
            dma(32),
            dma(CHUNKS * 8),
            dma(Z - 1),
            dma(X - 1),
            dma(G - 1),
        ],
        compiler_params=pltpu.CompilerParams(collective_id=0, has_side_effects=True),
    )(*args)


def body(
    inputs,
    norm_gain,
    w_query,
    w_forget,
    w_value,
    lower_bound,
    head_gain,
    w_out,
    prior_state,
    prev_forget,
    prev_values,
    accepted,
):
    mixed, base_state = fused(
        inputs.T,
        norm_gain.reshape(1, FEATS),
        w_query,
        w_forget,
        w_value,
        w_out.T,
        lower_bound.reshape(HEADS, HEAD),
        head_gain.reshape(HEADS, HEAD),
        prior_state,
        prev_forget,
        prev_values,
        accepted,
    )
    return (mixed.T, base_state)


def solution(mesh):
    split = Mesh(mesh.devices.reshape(Z, Y, C, X), KV_TP)
    placed = (
        P(None, KV),
        P(KV),
        P(KV, "tp"),
        P(KV, "tp"),
        P(KV, "tp"),
        P("tp"),
        P("tp"),
        P("tp", KV),
        P(KV, "tp", None, None),
        P(KV, None, "tp"),
        P(KV, None, "tp"),
        P(KV),
    )
    return jax.shard_map(
        body,
        mesh=split,
        in_specs=placed,
        out_specs=(P(None, KV_TP), P(KV, "tp", None, None)),
        check_vma=False,
    )
```

```python
import functools

import jax
import jax.numpy as jnp
from jax import lax
from jax.experimental import pallas as pl
from jax.experimental.pallas import tpu as pltpu
from jax.sharding import Mesh
from jax.sharding import PartitionSpec as P

KV = ("kv_0", "kv_1", "kv_2")
KV_TP = ("kv_0", "kv_1", "kv_2", "tp")
MESH_ID = pl.DeviceIdType.MESH
EPSILON = 1e-06
F32 = jnp.float32
BF16 = jnp.bfloat16

D = 4096
Z, Y, C, X = 8, 4, 2, 4
G = Y * C
FEATS = 64
OWN = 32
SET = Z * OWN
TOKENS = 2048
HEADS = 4
HEAD = 128
COLS = HEADS * HEAD
SEQS = 8
STEPS = 4
UP, DOWN = 0, 1
WIDE = 3 * HEAD
HOPS = ((4, 3), (3, 4), (4, 3), (3, 4))
MERGES = {4: ((4, 3), (2, 1)), 3: ((3, 2), (None, 1))}


def kernel(
    x_hbm,
    gain_ref,
    wq_hbm,
    wf_hbm,
    wv_hbm,
    wo_hbm,
    floor_ref,
    head_gain_ref,
    prior_hbm,
    prev_gate_ref,
    prev_value_ref,
    accepted_ref,
    out_ref,
    base_ref,
    x_raw,
    x_send,
    x_all,
    sq_send,
    sq_all,
    sq_mine,
    sq_z,
    w_all,
    wo_all,
    base_low,
    part,
    first_send,
    first_recv,
    second_send,
    second_recv,
    normed_all,
    final_send,
    final_recv,
    local_sem,
    x_sems,
    sq_sems,
    sqz_sems,
    w_sems,
    first_sems,
    second_sems,
    normed_sems,
    final_sems,
):
    z = lax.axis_index("kv_0")
    y = lax.axis_index("kv_1")
    c = lax.axis_index("kv_2")
    x = lax.axis_index("tp")
    g = y * C + c

    def at_z(step):
        return lax.rem(z + (step + Z), Z)

    def at_y(step):
        return lax.rem(y + (step + Y), Y)

    def at_x(step):
        return lax.rem(x + (step + X), X)

    sib = 1 - c
    group_steps = [(2, 0), (2, 1), (1, 0), (1, 1), (3, 0), (3, 1), (0, 1)]

    def group_peer(dy, dc):
        return at_y(dy), (sib if dc else c)

    barrier = pltpu.get_barrier_semaphore()
    peers = [(at_z(dz), y, c, x) for dz in (4, 3, 5, 2, 6, 1, 7)]
    for dy, dc in group_steps:
        py, pc = group_peer(dy, dc)
        peers.append((z, py, pc, x))
    for dx in range(1, X):
        peers.append((z, y, c, at_x(dx)))
    for peer in peers:
        pl.semaphore_signal(barrier, inc=1, device_id=peer, device_id_type=MESH_ID)

    x_load = pltpu.make_async_copy(x_hbm, x_raw, local_sem.at[0])
    x_load.start()
    w_loads = []
    for h in range(HEADS):
        loads = []
        for k, src in enumerate((wq_hbm, wf_hbm, wv_hbm)):
            load = pltpu.make_async_copy(
                src.at[:, pl.ds(h * HEAD, HEAD)],
                w_all.at[h, g, :, pl.ds(k * HEAD, HEAD)],
                local_sem.at[3 + h * 3 + k],
            )
            load.start()
            loads.append(load)
        w_loads.append(loads)
    wo_load = pltpu.make_async_copy(wo_hbm, wo_all.at[g], local_sem.at[1])
    wo_load.start()
    w_loads.append([wo_load])
    prior_load = pltpu.make_async_copy(prior_hbm, base_ref, local_sem.at[2])
    prior_load.start()

    gain_col = jnp.transpose(jnp.broadcast_to(gain_ref[...].astype(F32), (HEAD, FEATS)))
    lane_block = lax.broadcasted_iota(jnp.int32, (FEATS, HEAD), 1) // OWN
    x_load.wait()
    for peer in range(G):
        for half in range(2):
            tile = None
            for k in range(4):
                zz = half * 4 + k
                src = x_raw[:, pl.ds(zz * 256 + (peer // 4) * 128, 128)].astype(F32)
                shift = ((k - peer % 4) * OWN) % 128
                if shift:
                    src = pltpu.roll(src, shift, 1)
                tile = src if tile is None else jnp.where(lane_block == k, src, tile)
            lanes = pl.ds(half * 128, 128)
            sq_send[peer, :, lanes] = jnp.sum(tile * tile, axis=0, keepdims=True)
            x_send[peer, :, lanes] = (tile * gain_col).astype(BF16)

    pl.semaphore_wait(barrier, len(peers))

    def remote(src, dst, sems, index, peer):
        return pltpu.make_async_remote_copy(
            src_ref=src,
            dst_ref=dst,
            send_sem=sems.at[0, index],
            recv_sem=sems.at[1, index],
            device_id=peer,
            device_id_type=MESH_ID,
        )

    started = []

    def go(copy):
        copy.start()
        started.append(copy)
        return copy

    W = [{} for _ in range(HEADS + 1)]

    def w_slot(j, member):
        return w_all.at[j, member] if j < HEADS else wo_all.at[member]

    def w_out(j):
        for load in w_loads[j]:
            load.wait()
        own = w_slot(j, g)
        for i, dy in enumerate((2, 1, 3)):
            W[j][dy] = go(remote(own, own, w_sems, j * 7 + i, (z, at_y(dy), c, x)))
        W[j]["sib", 0] = go(remote(own, own, w_sems, j * 7 + 3, (z, y, sib, x)))

    def w_forward(j):
        for i, dy in enumerate((1, 3, 2)):
            W[j][dy].wait_recv()
            block = w_slot(j, at_y(-dy) * C + c)
            W[j]["sib", dy] = go(remote(block, block, w_sems, j * 7 + 4 + i, (z, y, sib, x)))

    def w_complete(j):
        for dy in (0, 1, 3, 2):
            W[j]["sib", dy].wait_recv()

    w_out(0)
    x_copies, sq_copies = [], []
    for i, (dy, dc) in enumerate(group_steps):
        py, pc = group_peer(dy, dc)
        pg = py * C + pc
        peer = (z, py, pc, x)
        x_copies.append(go(remote(x_send.at[pg], x_all.at[g], x_sems, i, peer)))
        sq_copies.append(go(remote(sq_send.at[pg], sq_all.at[g], sq_sems, i, peer)))
    for j in range(1, HEADS + 1):
        w_out(j)
    x_all[g] = x_send[g]
    sq_all[g] = sq_send[g]

    prior_load.wait()
    position = lax.broadcasted_iota(jnp.int32, (STEPS, COLS), 0)
    decays, keys_old, values_old = [], [], []
    for s in range(SEQS):
        taken = position < accepted_ref[s]
        gate = jnp.where(taken, prev_gate_ref[s], 1.0)
        key = 1.0 - gate
        after = jnp.ones((1, COLS), F32)
        rows = [None] * STEPS
        for j in reversed(range(STEPS)):
            rows[j] = key[j : j + 1] * after
            after = after * gate[j : j + 1]
        decays.append(after)
        keys_old.append(jnp.concatenate(rows, axis=0))
        values_old.append(prev_value_ref[s].astype(F32))
    for h in range(HEADS):
        cols = slice(h * HEAD, (h + 1) * HEAD)
        decay_cols = jnp.transpose(
            jnp.concatenate([decays[s][:, cols] for s in range(SEQS)], axis=0)
        )
        for s in range(SEQS):
            added = lax.dot_general(
                keys_old[s][:, cols],
                values_old[s][:, cols],
                (((0,), (0,)), ((), ())),
                precision=lax.Precision.HIGHEST,
                preferred_element_type=F32,
            )
            new = base_ref[s, h] * decay_cols[:, s : s + 1] + added
            base_ref[s, h] = new
            base_low[s, h] = new.astype(BF16)

    def squares_out():
        for copy in sq_copies:
            copy.wait_recv()
        total = sq_all[0]
        for k in range(1, G):
            total = total + sq_all[k]
        sq_mine[...] = total
        copies = []
        for dz in range(1, Z):
            peer = (at_z(dz), y, c, x)
            copies.append(go(remote(sq_mine, sq_z.at[z], sqz_sems, dz - 1, peer)))
        sq_z[z] = total
        return copies

    def token_scale(copies):
        for copy in copies:
            copy.wait_recv()
        squares = sq_z[0]
        for k in range(1, Z):
            squares = squares + sq_z[k]
        token = lax.broadcasted_iota(jnp.int32, (OWN, SET), 0) + z * OWN
        lane = lax.broadcasted_iota(jnp.int32, (OWN, SET), 1)
        own_squares = jnp.sum(
            jnp.where(lane == token, jnp.broadcast_to(squares, (OWN, SET)), 0.0),
            axis=1,
            keepdims=True,
        )
        return lax.rsqrt(own_squares / D + EPSILON)

    first, second = {}, {}

    def multiply(j, left):
        product = jnp.dot(left, w_all[j].reshape(G * FEATS, WIDE), preferred_element_type=F32)
        part[j] = product.reshape(Z, OWN, WIDE)
        for way, sign in ((UP, 1), (DOWN, -1)):
            for m, (far, near) in enumerate(MERGES[HOPS[j][way]]):
                index = (j * 2 + way) * 2 + m
                if far is None:
                    second_send[j, way, m] = part[j, at_z(sign * near)].astype(BF16)
                    src, dst, sems = second_send.at[j, way, m], second_recv.at[j, way, m], second_sems
                    second[j, way, m] = go(
                        remote(src, dst, sems, index, (at_z(sign * near), y, c, x))
                    )
                else:
                    first_send[j, way, m] = part[j, at_z(sign * far)].astype(BF16)
                    src, dst, sems = first_send.at[j, way, m], first_recv.at[j, way, m], first_sems
                    first[j, way, m] = go(remote(src, dst, sems, index, (at_z(sign), y, c, x)))

    def merge(j):
        for m in range(2):
            for way, sign in ((UP, 1), (DOWN, -1)):
                far, near = MERGES[HOPS[j][way]][m]
                if far is None:
                    continue
                first[j, way, m].wait_recv()
                value = part[j, at_z(sign * near)] + first_recv[j, way, m].astype(F32)
                second_send[j, way, m] = value.astype(BF16)
                src, dst = second_send.at[j, way, m], second_recv.at[j, way, m]
                index = (j * 2 + way) * 2 + m
                second[j, way, m] = go(
                    remote(src, dst, second_sems, index, (at_z(sign * near), y, c, x))
                )

    row = lax.broadcasted_iota(jnp.int32, (OWN, HEAD), 0)
    when = lax.rem(row, STEPS)
    first_seq = lax.broadcasted_iota(jnp.int32, (8, HEAD), 0) < STEPS
    normed_copies = []

    def recur(h, rscale):
        total = part[h, z]
        for way in (UP, DOWN):
            for m in range(2):
                second[h, way, m].wait_recv()
                total = total + second_recv[h, way, m].astype(F32)
        total = total * rscale
        floor = floor_ref[h : h + 1, :]
        gate = floor + (1.0 - floor) * jax.nn.sigmoid(total[:, HEAD : 2 * HEAD])
        key = 1.0 - gate
        pre = total[:, :HEAD]
        query = pre * jax.nn.sigmoid(pre)
        value = total[:, 2 * HEAD :]
        decayed = query
        result = jnp.sum(query * key, axis=1, keepdims=True) * value
        for back in range(1, STEPS):
            gate_back = gate if back == 1 else pltpu.roll(gate, back - 1, 0)
            decayed = decayed * (
                gate_back if back == 1 else jnp.where(when >= back - 1, gate_back, 1.0)
            )
            weight = jnp.sum(
                jnp.where(when >= back, decayed * pltpu.roll(key, back, 0), 0.0),
                axis=1,
                keepdims=True,
            )
            result = result + weight * pltpu.roll(value, back, 0)
        decayed = decayed * jnp.where(when >= STEPS - 1, pltpu.roll(gate, STEPS - 1, 0), 1.0)
        low = decayed.astype(BF16)
        carried = []
        for pair in range(SEQS // 2):
            rows = low[pair * 8 : pair * 8 + 8]
            one = jnp.dot(rows, base_low[2 * pair, h], preferred_element_type=F32)
            two = jnp.dot(rows, base_low[2 * pair + 1, h], preferred_element_type=F32)
            carried.append(jnp.where(first_seq, one, two))
        result = result + jnp.concatenate(carried, axis=0)
        mean = jnp.sum(result * result, axis=1, keepdims=True) / HEAD
        normed = result * lax.rsqrt(mean + EPSILON) * head_gain_ref[h : h + 1, :]
        normed_all[z, h] = normed.astype(BF16)
        slot = normed_all.at[z, h]
        for i, dz in enumerate((4, 3, 5, 2, 6, 1, 7)):
            normed_copies.append(
                go(remote(slot, slot, normed_sems, h * 7 + i, (at_z(dz), y, c, x)))
            )

    w_forward(0)
    w_complete(0)
    sqz_copies = squares_out()
    for copy in x_copies:
        copy.wait_recv()
    left = jnp.transpose(x_all[...].reshape(G * FEATS, SET))
    multiply(0, left)
    w_forward(1)
    merge(0)
    w_complete(1)
    multiply(1, left)
    w_forward(2)
    w_complete(2)
    multiply(2, left)
    merge(1)
    w_forward(3)
    w_complete(3)
    multiply(3, left)
    rscale = token_scale(sqz_copies)
    recur(0, rscale)
    merge(2)
    merge(3)
    recur(1, rscale)
    w_forward(4)
    recur(2, rscale)
    recur(3, rscale)
    w_complete(4)

    for copy in normed_copies:
        copy.wait_recv()

    product = None
    for h in range(HEADS):
        term = lax.dot_general(
            wo_all[:, :, pl.ds(h * HEAD, HEAD)].reshape(G * FEATS, HEAD),
            normed_all[:, h].reshape(SET, HEAD),
            (((1,), (1,)), ((), ())),
            preferred_element_type=F32,
        )
        product = term if product is None else product + term
    final_send[...] = product.astype(BF16).reshape(G, X, FEATS // X, SET)
    copies = []
    final_recv[x, g] = final_send[g, x]
    for i, (dy, dc, dx) in enumerate(
        [(dy, dc, dx) for dy in (2, 1, 3, 0) for dx in (2, 1, 3, 0) for dc in (0, 1) if dy or dx or dc]
    ):
        py, pc = group_peer(dy, dc)
        px = at_x(dx)
        src, dst = final_send.at[py * C + pc, px], final_recv.at[x, g]
        copies.append(go(remote(src, dst, final_sems, i, (z, py, pc, px))))
    for copy in copies:
        copy.wait_recv()

    rows_out = FEATS // X
    for k in range(G):
        total = final_recv[0, k].astype(F32)
        for m in range(1, X):
            total = total + final_recv[m, k].astype(F32)
        out_ref[k] = total.astype(BF16)

    for copy in started:
        copy.wait_send()


def tail(pieces_ref, base_ref, out_ref, base_hbm, sems):
    stores = []
    for s in range(SEQS):
        store = pltpu.make_async_copy(base_ref.at[s], base_hbm.at[s], sems.at[s])
        store.start()
        stores.append(store)
    rows_out = FEATS // X
    lane_block = lax.broadcasted_iota(jnp.int32, (rows_out, HEAD), 1) // OWN
    for zz in range(Z):
        for half_g in range(2):
            tile = None
            for k in range(4):
                src = pieces_ref[half_g * 4 + k, :, pl.ds((zz // 4) * 128, 128)].astype(F32)
                shift = ((k - zz % 4) * OWN) % 128
                if shift:
                    src = pltpu.roll(src, shift, 1)
                tile = src if tile is None else jnp.where(lane_block == k, src, tile)
            out_ref[:, pl.ds(zz * 256 + half_g * 128, 128)] = tile.astype(BF16)
    for store in stores:
        store.wait()


def fused(*args):
    any_space = pl.BlockSpec(memory_space=pl.ANY)
    vmem = pl.BlockSpec(memory_space=pltpu.VMEM)
    smem = pl.BlockSpec(memory_space=pltpu.SMEM)
    dma = lambda n: pltpu.SemaphoreType.DMA((2, n))
    pieces, base = pl.pallas_call(
        kernel,
        out_shape=(
            pltpu.VMEM((G, FEATS // X, SET), BF16),
            pltpu.VMEM((SEQS, HEADS, HEAD, HEAD), F32),
        ),
        in_specs=[any_space, vmem] + [any_space] * 4 + [vmem, vmem, any_space, vmem, vmem, smem],
        out_specs=(vmem, vmem),
        scratch_shapes=[
            pltpu.VMEM((FEATS, TOKENS), BF16),
            pltpu.VMEM((G, FEATS, SET), BF16),
            pltpu.VMEM((G, FEATS, SET), BF16),
            pltpu.VMEM((G, 1, SET), F32),
            pltpu.VMEM((G, 1, SET), F32),
            pltpu.VMEM((1, SET), F32),
            pltpu.VMEM((Z, 1, SET), F32),
            pltpu.VMEM((HEADS, G, FEATS, WIDE), BF16),
            pltpu.VMEM((G, FEATS, COLS), BF16),
            pltpu.VMEM((SEQS, HEADS, HEAD, HEAD), BF16),
            pltpu.VMEM((HEADS, Z, OWN, WIDE), F32),
            pltpu.VMEM((HEADS, 2, 2, OWN, WIDE), BF16),
            pltpu.VMEM((HEADS, 2, 2, OWN, WIDE), BF16),
            pltpu.VMEM((HEADS, 2, 2, OWN, WIDE), BF16),
            pltpu.VMEM((HEADS, 2, 2, OWN, WIDE), BF16),
            pltpu.VMEM((Z, HEADS, OWN, HEAD), BF16),
            pltpu.VMEM((G, X, FEATS // X, SET), BF16),
            pltpu.VMEM((X, G, FEATS // X, SET), BF16),
            pltpu.SemaphoreType.DMA((15,)),
            dma(G - 1),
            dma(G - 1),
            dma(Z - 1),
            dma((HEADS + 1) * 7),
            dma(HEADS * 4),
            dma(HEADS * 4),
            dma(HEADS * 7),
            dma(G * X - 1),
        ],
        compiler_params=pltpu.CompilerParams(collective_id=0, has_side_effects=True),
    )(*args)
    return pl.pallas_call(
        tail,
        out_shape=(
            jax.ShapeDtypeStruct((FEATS // X, TOKENS), BF16),
            jax.ShapeDtypeStruct((SEQS, HEADS, HEAD, HEAD), F32),
        ),
        in_specs=[vmem, vmem],
        out_specs=(vmem, any_space),
        scratch_shapes=[pltpu.SemaphoreType.DMA((SEQS,))],
        compiler_params=pltpu.CompilerParams(vmem_limit_bytes=8 * 2**20),
    )(pieces, base)


def body(
    inputs,
    norm_gain,
    w_query,
    w_forget,
    w_value,
    lower_bound,
    head_gain,
    w_out,
    prior_state,
    prev_forget,
    prev_values,
    accepted,
):
    mixed, base_state = fused(
        inputs.T,
        norm_gain.reshape(1, FEATS),
        w_query,
        w_forget,
        w_value,
        w_out.T,
        lower_bound.reshape(HEADS, HEAD),
        head_gain.reshape(HEADS, HEAD),
        prior_state,
        prev_forget,
        prev_values,
        accepted,
    )
    return (mixed.T, base_state)


def solution(mesh):
    split = Mesh(mesh.devices.reshape(Z, Y, C, X), KV_TP)
    placed = (
        P(None, KV),
        P(KV),
        P(KV, "tp"),
        P(KV, "tp"),
        P(KV, "tp"),
        P("tp"),
        P("tp"),
        P("tp", KV),
        P(KV, "tp", None, None),
        P(KV, None, "tp"),
        P(KV, None, "tp"),
        P(KV),
    )
    return jax.shard_map(
        body,
        mesh=split,
        in_specs=placed,
        out_specs=(P(None, KV_TP), P(KV, "tp", None, None)),
        check_vma=False,
    )
```

```python
import functools

import jax
import jax.numpy as jnp
from jax import lax
from jax.experimental import pallas as pl
from jax.experimental.pallas import tpu as pltpu
from jax.sharding import Mesh
from jax.sharding import PartitionSpec as P

KV = ("kv_0", "kv_1", "kv_2")
KV_TP = ("kv_0", "kv_1", "kv_2", "tp")
MESH_ID = pl.DeviceIdType.MESH
EPSILON = 1e-06
F32 = jnp.float32
BF16 = jnp.bfloat16

D = 4096
Z, Y, C, X = 8, 4, 2, 4
G = Y * C
FEATS = 64
OWN = 32
SET = Z * OWN
TOKENS = 2048
HEADS = 4
HEAD = 128
COLS = HEADS * HEAD
SEQS = 8
STEPS = 4
UP, DOWN = 0, 1
WIDE = 3 * HEAD
HOPS = ((4, 3), (3, 4), (4, 3), (3, 4))
MERGES = {4: ((4, 3), (2, 1)), 3: ((3, 2), (None, 1))}


def kernel(
    x_hbm,
    gain_hbm,
    wq_hbm,
    wf_hbm,
    wv_hbm,
    wo_hbm,
    floor_hbm,
    head_gain_hbm,
    prior_hbm,
    prev_gate_hbm,
    prev_value_hbm,
    accepted_hbm,
    out_ref,
    base_ref,
    gain_ref,
    floor_ref,
    head_gain_ref,
    prev_gate_ref,
    prev_value_ref,
    accepted_ref,
    x_raw,
    x_send,
    x_all,
    left_ref,
    sq_send,
    sq_all,
    sq_mine,
    sq_z,
    w_all,
    wo_all,
    base_low,
    part,
    first_send,
    first_recv,
    second_send,
    second_recv,
    normed_all,
    final_send,
    final_recv,
    relay_sem,
    local_sem,
    x_sems,
    sq_sems,
    sqz_sems,
    w_sems,
    first_sems,
    second_sems,
    normed_sems,
    final_sems,
):
    z = lax.axis_index("kv_0")
    y = lax.axis_index("kv_1")
    c = lax.axis_index("kv_2")
    x = lax.axis_index("tp")
    g = y * C + c

    def at_z(step):
        return lax.rem(z + (step + Z), Z)

    def at_y(step):
        return lax.rem(y + (step + Y), Y)

    def at_x(step):
        return lax.rem(x + (step + X), X)

    sib = 1 - c
    group_steps = [(2, 0), (2, 1), (1, 0), (1, 1), (3, 0), (3, 1), (0, 1)]

    def group_peer(dy, dc):
        return at_y(dy), (sib if dc else c)

    barrier = pltpu.get_barrier_semaphore()
    z_near = [(at_z(1), y, c, x), (at_z(-1), y, c, x)]
    peers = []
    for dy, dc in group_steps:
        py, pc = group_peer(dy, dc)
        peers.append((z, py, pc, x))
    for dx in (2, 1, 3):
        peers.append((z, y, c, at_x(dx)))
    for peer in peers + z_near:
        pl.semaphore_signal(barrier, inc=1, device_id=peer, device_id_type=MESH_ID)

    def load(src, dst, index):
        copy = pltpu.make_async_copy(src, dst, local_sem.at[index])
        copy.start()
        return copy

    def load_weights(h):
        return [
            load(
                src.at[:, pl.ds(h * HEAD, HEAD)],
                w_all.at[h, 0, 0, :, pl.ds(k * HEAD, HEAD)],
                3 + h * 3 + k,
            )
            for k, src in enumerate((wq_hbm, wf_hbm, wv_hbm))
        ]

    w_loads = [load_weights(0)]
    x_load = load(x_hbm, x_raw, 0)
    gain_load = load(gain_hbm, gain_ref, 15)
    w_loads += [load_weights(h) for h in range(1, HEADS)]
    base_loads = [
        load(prior_hbm, base_ref, 2),
        load(prev_gate_hbm, prev_gate_ref, 18),
        load(prev_value_hbm, prev_value_ref, 19),
        load(accepted_hbm, accepted_ref, 20),
    ]
    small_loads = [load(floor_hbm, floor_ref, 16), load(head_gain_hbm, head_gain_ref, 17)]
    w_loads.append([load(wo_hbm, wo_all.at[0, 0], 1)])

    for copy in w_loads[0]:
        copy.wait()
    pl.semaphore_wait(barrier, len(peers + z_near))

    def relay_out(k):
        for peer in z_near:
            pl.semaphore_signal(relay_sem.at[k], inc=1, device_id=peer, device_id_type=MESH_ID)

    def relay_in(k):
        pl.semaphore_wait(relay_sem.at[k], 2)

    relay_out(0)

    def remote(src, dst, sems, index, peer):
        return pltpu.make_async_remote_copy(
            src_ref=src,
            dst_ref=dst,
            send_sem=sems.at[0, index],
            recv_sem=sems.at[1, index],
            device_id=peer,
            device_id_type=MESH_ID,
        )

    started = []

    def go(copy):
        copy.start()
        started.append(copy)
        return copy

    W = [{} for _ in range(HEADS + 1)]

    def w_slot(j, dy, dc):
        return w_all.at[j, dy, dc] if j < HEADS else wo_all.at[dy, dc]

    def w_out(j):
        own = w_slot(j, 0, 0)
        for i, dy in enumerate((2, 1, 3)):
            W[j][dy] = go(remote(own, w_slot(j, dy, 0), w_sems, j * 7 + i, (z, at_y(dy), c, x)))
        W[j]["sib", 0] = go(remote(own, w_slot(j, 0, 1), w_sems, j * 7 + 3, (z, y, sib, x)))

    def w_forward(j):
        for i, dy in enumerate((1, 3, 2)):
            W[j][dy].wait_recv()
            src, dst = w_slot(j, dy, 0), w_slot(j, dy, 1)
            W[j]["sib", dy] = go(remote(src, dst, w_sems, j * 7 + 4 + i, (z, y, sib, x)))

    def w_complete(j):
        for dy in (0, 1, 3, 2):
            W[j]["sib", dy].wait_recv()

    w_out(0)

    x_load.wait()
    gain_load.wait()
    gain_col = jnp.transpose(jnp.broadcast_to(gain_ref[...].astype(F32), (HEAD, FEATS)))
    lane_block = lax.broadcasted_iota(jnp.int32, (FEATS, HEAD), 1) // OWN
    for peer in range(G):
        for half in range(2):
            tile = None
            for k in range(4):
                zz = half * 4 + k
                src = x_raw[:, pl.ds(zz * 256 + (peer // 4) * 128, 128)].astype(F32)
                shift = ((k - peer % 4) * OWN) % 128
                if shift:
                    src = pltpu.roll(src, shift, 1)
                tile = src if tile is None else jnp.where(lane_block == k, src, tile)
            lanes = pl.ds(half * 128, 128)
            sq_send[peer, :, lanes] = jnp.sum(tile * tile, axis=0, keepdims=True)
            x_send[peer, :, lanes] = (tile * gain_col).astype(BF16)
    X_in = {}
    sq_copies = []
    for i, (dy, dc) in enumerate(group_steps):
        py, pc = group_peer(dy, dc)
        pg = py * C + pc
        peer = (z, py, pc, x)
        X_in[dy, dc] = go(remote(x_send.at[pg], x_all.at[dy, dc], x_sems, i, peer))
        sq_copies.append(go(remote(sq_send.at[pg], sq_all.at[i], sq_sems, i, peer)))
    for j in range(1, HEADS + 1):
        for copy in w_loads[j]:
            copy.wait()
        w_out(j)
    x_all[0, 0] = x_send[g]

    for copy in base_loads:
        copy.wait()
    position = lax.broadcasted_iota(jnp.int32, (STEPS, COLS), 0)
    decays, keys_old, values_old = [], [], []
    for s in range(SEQS):
        taken = position < accepted_ref[s]
        gate = jnp.where(taken, prev_gate_ref[s], 1.0)
        key = 1.0 - gate
        after = jnp.ones((1, COLS), F32)
        rows = [None] * STEPS
        for j in reversed(range(STEPS)):
            rows[j] = key[j : j + 1] * after
            after = after * gate[j : j + 1]
        decays.append(after)
        keys_old.append(jnp.concatenate(rows, axis=0))
        values_old.append(prev_value_ref[s].astype(F32))
    for h in range(HEADS):
        cols = slice(h * HEAD, (h + 1) * HEAD)
        decay_cols = jnp.transpose(
            jnp.concatenate([decays[s][:, cols] for s in range(SEQS)], axis=0)
        )
        for s in range(SEQS):
            added = lax.dot_general(
                keys_old[s][:, cols],
                values_old[s][:, cols],
                (((0,), (0,)), ((), ())),
                precision=lax.Precision.HIGHEST,
                preferred_element_type=F32,
            )
            new = base_ref[s, h] * decay_cols[:, s : s + 1] + added
            base_ref[s, h] = new
            base_low[s, h] = new.astype(BF16)

    def squares_out():
        for copy in sq_copies:
            copy.wait_recv()
        total = sq_send[g]
        for k in range(G - 1):
            total = total + sq_all[k]
        sq_mine[...] = total
        copies = []
        for dz in range(1, Z):
            peer = (at_z(dz), y, c, x)
            copies.append(go(remote(sq_mine, sq_z.at[z], sqz_sems, dz - 1, peer)))
        sq_z[z] = total
        return copies

    def token_scale(copies):
        for copy in copies:
            copy.wait_recv()
        squares = sq_z[0]
        for k in range(1, Z):
            squares = squares + sq_z[k]
        token = lax.broadcasted_iota(jnp.int32, (OWN, SET), 0) + z * OWN
        lane = lax.broadcasted_iota(jnp.int32, (OWN, SET), 1)
        own_squares = jnp.sum(
            jnp.where(lane == token, jnp.broadcast_to(squares, (OWN, SET)), 0.0),
            axis=1,
            keepdims=True,
        )
        return lax.rsqrt(own_squares / D + EPSILON)

    first, second = {}, {}

    def inputs_in():
        for dy in (0, 1, 3, 2):
            for dc in range(C):
                if dy or dc:
                    X_in[dy, dc].wait_recv()
            block = x_all[dy].reshape(C * FEATS, SET)
            left_ref[:, pl.ds(dy * C * FEATS, C * FEATS)] = jnp.transpose(block)

    def multiply(j):
        product = jnp.dot(
            left_ref[...], w_all[j].reshape(G * FEATS, WIDE), preferred_element_type=F32
        )
        part[j] = product.reshape(Z, OWN, WIDE)
        for way, sign in ((UP, 1), (DOWN, -1)):
            for m, (far, near) in enumerate(MERGES[HOPS[j][way]]):
                index = (j * 2 + way) * 2 + m
                if far is None:
                    second_send[j, way, m] = part[j, at_z(sign * near)].astype(BF16)
                    src, dst, sems = second_send.at[j, way, m], second_recv.at[j, way, m], second_sems
                    second[j, way, m] = go(
                        remote(src, dst, sems, index, (at_z(sign * near), y, c, x))
                    )
                else:
                    first_send[j, way, m] = part[j, at_z(sign * far)].astype(BF16)
                    src, dst, sems = first_send.at[j, way, m], first_recv.at[j, way, m], first_sems
                    first[j, way, m] = go(remote(src, dst, sems, index, (at_z(sign), y, c, x)))

    def merge(j):
        for m in range(2):
            for way, sign in ((UP, 1), (DOWN, -1)):
                far, near = MERGES[HOPS[j][way]][m]
                if far is None:
                    continue
                first[j, way, m].wait_recv()
                value = part[j, at_z(sign * near)] + first_recv[j, way, m].astype(F32)
                second_send[j, way, m] = value.astype(BF16)
                src, dst = second_send.at[j, way, m], second_recv.at[j, way, m]
                index = (j * 2 + way) * 2 + m
                second[j, way, m] = go(
                    remote(src, dst, second_sems, index, (at_z(sign * near), y, c, x))
                )

    row = lax.broadcasted_iota(jnp.int32, (OWN, HEAD), 0)
    when = lax.rem(row, STEPS)
    first_seq = lax.broadcasted_iota(jnp.int32, (8, HEAD), 0) < STEPS
    normed_copies = [[] for _ in range(HEADS)]

    def recur(h, rscale):
        total = part[h, z]
        for way in (UP, DOWN):
            for m in range(2):
                second[h, way, m].wait_recv()
                total = total + second_recv[h, way, m].astype(F32)
        total = total * rscale
        floor = floor_ref[h : h + 1, :]
        gate = floor + (1.0 - floor) * jax.nn.sigmoid(total[:, HEAD : 2 * HEAD])
        key = 1.0 - gate
        pre = total[:, :HEAD]
        query = pre * jax.nn.sigmoid(pre)
        value = total[:, 2 * HEAD :]
        decayed = query
        result = jnp.sum(query * key, axis=1, keepdims=True) * value
        for back in range(1, STEPS):
            gate_back = gate if back == 1 else pltpu.roll(gate, back - 1, 0)
            decayed = decayed * (
                gate_back if back == 1 else jnp.where(when >= back - 1, gate_back, 1.0)
            )
            weight = jnp.sum(
                jnp.where(when >= back, decayed * pltpu.roll(key, back, 0), 0.0),
                axis=1,
                keepdims=True,
            )
            result = result + weight * pltpu.roll(value, back, 0)
        decayed = decayed * jnp.where(when >= STEPS - 1, pltpu.roll(gate, STEPS - 1, 0), 1.0)
        low = decayed.astype(BF16)
        carried = []
        for pair in range(SEQS // 2):
            rows = low[pair * 8 : pair * 8 + 8]
            one = jnp.dot(rows, base_low[2 * pair, h], preferred_element_type=F32)
            two = jnp.dot(rows, base_low[2 * pair + 1, h], preferred_element_type=F32)
            carried.append(jnp.where(first_seq, one, two))
        result = result + jnp.concatenate(carried, axis=0)
        mean = jnp.sum(result * result, axis=1, keepdims=True) / HEAD
        normed = result * lax.rsqrt(mean + EPSILON) * head_gain_ref[h : h + 1, :]
        normed_all[z, h] = normed.astype(BF16)
        slot = normed_all.at[z, h]
        for i, dz in enumerate((4, 3, 5, 2, 6, 1, 7)):
            normed_copies[h].append(
                go(remote(slot, slot, normed_sems, h * 7 + i, (at_z(dz), y, c, x)))
            )

    relay_in(0)
    relay_out(1)
    w_forward(0)
    relay_in(1)
    relay_out(2)
    w_complete(0)
    inputs_in()
    multiply(0)
    relay_in(2)
    sqz_copies = squares_out()
    for copy in small_loads:
        copy.wait()
    w_forward(1)
    merge(0)
    w_complete(1)
    multiply(1)
    w_forward(2)
    w_complete(2)
    multiply(2)
    w_forward(3)
    w_complete(3)
    multiply(3)
    merge(1)
    rscale = token_scale(sqz_copies)
    merge(2)
    merge(3)
    recur(0, rscale)
    recur(1, rscale)
    w_forward(4)
    recur(2, rscale)
    recur(3, rscale)
    w_complete(4)

    product = None
    for h in range(HEADS):
        for copy in normed_copies[h]:
            copy.wait_recv()
        term = lax.dot_general(
            wo_all[:, :, :, pl.ds(h * HEAD, HEAD)].reshape(G * FEATS, HEAD),
            normed_all[:, h].reshape(SET, HEAD),
            (((1,), (1,)), ((), ())),
            preferred_element_type=F32,
        )
        product = term if product is None else product + term
    final_send[...] = product.astype(BF16).reshape(Y, C, X, FEATS // X, SET)
    copies = []
    final_recv[x, g] = final_send[0, 0, x]
    for i, (dy, dc, dx) in enumerate(
        [(dy, dc, dx) for dy in (2, 1, 3, 0) for dx in (2, 1, 3, 0) for dc in (0, 1) if dy or dx or dc]
    ):
        py, pc = at_y(-dy), (sib if dc else c)
        px = at_x(dx)
        src, dst = final_send.at[dy, dc, px], final_recv.at[x, g]
        copies.append(go(remote(src, dst, final_sems, i, (z, py, pc, px))))
    for copy in copies:
        copy.wait_recv()

    rows_out = FEATS // X
    for k in range(G):
        total = final_recv[0, k].astype(F32)
        for m in range(1, X):
            total = total + final_recv[m, k].astype(F32)
        out_ref[k] = total.astype(BF16)

    for copy in started:
        copy.wait_send()


def tail(pieces_ref, base_ref, out_ref, base_hbm, sems):
    stores = []
    for s in range(SEQS):
        store = pltpu.make_async_copy(base_ref.at[s], base_hbm.at[s], sems.at[s])
        store.start()
        stores.append(store)
    rows_out = FEATS // X
    lane_block = lax.broadcasted_iota(jnp.int32, (rows_out, HEAD), 1) // OWN
    for zz in range(Z):
        for half_g in range(2):
            tile = None
            for k in range(4):
                src = pieces_ref[half_g * 4 + k, :, pl.ds((zz // 4) * 128, 128)].astype(F32)
                shift = ((k - zz % 4) * OWN) % 128
                if shift:
                    src = pltpu.roll(src, shift, 1)
                tile = src if tile is None else jnp.where(lane_block == k, src, tile)
            out_ref[:, pl.ds(zz * 256 + half_g * 128, 128)] = tile.astype(BF16)
    for store in stores:
        store.wait()


def fused(*args):
    any_space = pl.BlockSpec(memory_space=pl.ANY)
    vmem = pl.BlockSpec(memory_space=pltpu.VMEM)
    dma = lambda n: pltpu.SemaphoreType.DMA((2, n))
    pieces, base = pl.pallas_call(
        kernel,
        out_shape=(
            pltpu.VMEM((G, FEATS // X, SET), BF16),
            pltpu.VMEM((SEQS, HEADS, HEAD, HEAD), F32),
        ),
        in_specs=[any_space] * 12,
        out_specs=(vmem, vmem),
        scratch_shapes=[
            pltpu.VMEM((1, FEATS), BF16),
            pltpu.VMEM((HEADS, HEAD), F32),
            pltpu.VMEM((HEADS, HEAD), F32),
            pltpu.VMEM((SEQS, STEPS, COLS), F32),
            pltpu.VMEM((SEQS, STEPS, COLS), BF16),
            pltpu.SMEM((SEQS,), jnp.int32),
            pltpu.VMEM((FEATS, TOKENS), BF16),
            pltpu.VMEM((G, FEATS, SET), BF16),
            pltpu.VMEM((Y, C, FEATS, SET), BF16),
            pltpu.VMEM((SET, G * FEATS), BF16),
            pltpu.VMEM((G, 1, SET), F32),
            pltpu.VMEM((G - 1, 1, SET), F32),
            pltpu.VMEM((1, SET), F32),
            pltpu.VMEM((Z, 1, SET), F32),
            pltpu.VMEM((HEADS, Y, C, FEATS, WIDE), BF16),
            pltpu.VMEM((Y, C, FEATS, COLS), BF16),
            pltpu.VMEM((SEQS, HEADS, HEAD, HEAD), BF16),
            pltpu.VMEM((HEADS, Z, OWN, WIDE), F32),
            pltpu.VMEM((HEADS, 2, 2, OWN, WIDE), BF16),
            pltpu.VMEM((HEADS, 2, 2, OWN, WIDE), BF16),
            pltpu.VMEM((HEADS, 2, 2, OWN, WIDE), BF16),
            pltpu.VMEM((HEADS, 2, 2, OWN, WIDE), BF16),
            pltpu.VMEM((Z, HEADS, OWN, HEAD), BF16),
            pltpu.VMEM((Y, C, X, FEATS // X, SET), BF16),
            pltpu.VMEM((X, G, FEATS // X, SET), BF16),
            pltpu.SemaphoreType.REGULAR((3,)),
            pltpu.SemaphoreType.DMA((21,)),
            dma(G - 1),
            dma(G - 1),
            dma(Z - 1),
            dma((HEADS + 1) * 7),
            dma(HEADS * 4),
            dma(HEADS * 4),
            dma(HEADS * 7),
            dma(G * X - 1),
        ],
        compiler_params=pltpu.CompilerParams(collective_id=0, has_side_effects=True),
    )(*args)
    return pl.pallas_call(
        tail,
        out_shape=(
            jax.ShapeDtypeStruct((FEATS // X, TOKENS), BF16),
            jax.ShapeDtypeStruct((SEQS, HEADS, HEAD, HEAD), F32),
        ),
        in_specs=[vmem, vmem],
        out_specs=(vmem, any_space),
        scratch_shapes=[pltpu.SemaphoreType.DMA((SEQS,))],
        compiler_params=pltpu.CompilerParams(vmem_limit_bytes=8 * 2**20),
    )(pieces, base)


def body(
    inputs,
    norm_gain,
    w_query,
    w_forget,
    w_value,
    lower_bound,
    head_gain,
    w_out,
    prior_state,
    prev_forget,
    prev_values,
    accepted,
):
    mixed, base_state = fused(
        inputs.T,
        norm_gain.reshape(1, FEATS),
        w_query,
        w_forget,
        w_value,
        w_out.T,
        lower_bound.reshape(HEADS, HEAD),
        head_gain.reshape(HEADS, HEAD),
        prior_state,
        prev_forget,
        prev_values,
        accepted,
    )
    return (mixed.T, base_state)


def solution(mesh):
    split = Mesh(mesh.devices.reshape(Z, Y, C, X), KV_TP)
    placed = (
        P(None, KV),
        P(KV),
        P(KV, "tp"),
        P(KV, "tp"),
        P(KV, "tp"),
        P("tp"),
        P("tp"),
        P("tp", KV),
        P(KV, "tp", None, None),
        P(KV, None, "tp"),
        P(KV, None, "tp"),
        P(KV),
    )
    return jax.shard_map(
        body,
        mesh=split,
        in_specs=placed,
        out_specs=(P(None, KV_TP), P(KV, "tp", None, None)),
        check_vma=False,
    )
```

```python
import functools

import jax
import jax.numpy as jnp
from jax import lax
from jax.experimental import pallas as pl
from jax.experimental.pallas import tpu as pltpu
from jax.sharding import Mesh
from jax.sharding import PartitionSpec as P

KV = ("kv_0", "kv_1", "kv_2")
KV_TP = ("kv_0", "kv_1", "kv_2", "tp")
MESH_ID = pl.DeviceIdType.MESH
EPSILON = 1e-06
F32 = jnp.float32
BF16 = jnp.bfloat16

D = 4096
Z, Y, C, X = 8, 4, 2, 4
G = Y * C
FEATS = 64
OWN = 32
SET = Z * OWN
TOKENS = 2048
HEADS = 4
HEAD = 128
COLS = HEADS * HEAD
SEQS = 8
STEPS = 4
UP, DOWN = 0, 1
WIDE = 3 * HEAD
CHUNKS = ((0, 384), (384, 384), (768, 384), (1152, 384))
HOPS = ((4, 3), (3, 4), (4, 3), (3, 4))
SLOT = (0, 1, 3, 2)
MERGES = {4: ((4, 3), (2, 1)), 3: ((3, 2), (None, 1))}
KINDS = 10
ARRIVALS = 36


def kernel(
    x_hbm,
    gain_hbm,
    wq_hbm,
    wf_hbm,
    wv_hbm,
    wo_hbm,
    floor_hbm,
    head_gain_hbm,
    prior_hbm,
    prev_gate_hbm,
    prev_value_hbm,
    accepted_hbm,
    out_ref,
    base_ref,
    gain_ref,
    floor_ref,
    head_gain_ref,
    prev_gate_ref,
    prev_value_ref,
    accepted_ref,
    x_raw,
    x_send,
    x_all,
    left_ref,
    half_send,
    half_recv,
    sq_send,
    sq_all,
    sq_mine,
    sq_z,
    w_all,
    wo_all,
    base_low,
    part,
    first_send,
    first_recv,
    second_send,
    second_recv,
    normed_all,
    final_send,
    final_recv,
    relay_sem,
    local_sem,
    send_sems,
    recv_sems,
):
    z = lax.axis_index("kv_0")
    y = lax.axis_index("kv_1")
    c = lax.axis_index("kv_2")
    x = lax.axis_index("tp")
    g = y * C + c

    def at_z(step):
        return lax.rem(z + (step + Z), Z)

    def at_y(step):
        return lax.rem(y + (step + Y), Y)

    def at_x(step):
        return lax.rem(x + (step + X), X)

    sib = 1 - c
    group_steps = [(2, 0), (2, 1), (1, 0), (1, 1), (3, 0), (3, 1), (0, 1)]

    def group_peer(dy, dc):
        return at_y(dy), (sib if dc else c)

    barrier = pltpu.get_barrier_semaphore()
    z_near = [(at_z(1), y, c, x), (at_z(-1), y, c, x)]
    peers = []
    for dy, dc in group_steps:
        py, pc = group_peer(dy, dc)
        peers.append((z, py, pc, x))
    for dx in (2, 1, 3):
        peers.append((z, y, c, at_x(dx)))
    for peer in peers + z_near:
        pl.semaphore_signal(barrier, inc=1, device_id=peer, device_id_type=MESH_ID)

    def load(src, dst, index):
        copy = pltpu.make_async_copy(src, dst, local_sem.at[index])
        copy.start()
        return copy

    def load_weights(j):
        start, width = CHUNKS[j]
        for k in range(start // HEAD, (start + width) // HEAD):
            src = (wq_hbm, wf_hbm, wv_hbm)[k % 3].at[:, pl.ds(k // 3 * HEAD, HEAD)]
            load(src, w_all.at[0, :, pl.ds(k * HEAD, HEAD)], j)
        own = w_all.at[0, :, pl.ds(start, width)]
        return [pltpu.make_async_copy(own, own, local_sem.at[j])]

    w_loads = [load_weights(0)]
    x_load = load(x_hbm, x_raw, 4)
    gain_load = load(gain_hbm, gain_ref, 5)
    w_loads += [load_weights(j) for j in range(1, len(CHUNKS))]
    base_loads = [
        load(prior_hbm, base_ref, 6),
        load(prev_gate_hbm, prev_gate_ref, 7),
        load(prev_value_hbm, prev_value_ref, 8),
        load(accepted_hbm, accepted_ref, 9),
    ]
    small_loads = [load(floor_hbm, floor_ref, 10), load(head_gain_hbm, head_gain_ref, 11)]
    w_loads.append([load(wo_hbm, wo_all.at[0], 12)])

    x_load.wait()
    gain_load.wait()
    gain_col = jnp.transpose(jnp.broadcast_to(gain_ref[...].astype(F32), (HEAD, FEATS)))
    lane_block = lax.broadcasted_iota(jnp.int32, (FEATS, HEAD), 1) // OWN
    for peer in range(G):
        for half in range(2):
            tile = None
            for k in range(4):
                zz = half * 4 + k
                src = x_raw[:, pl.ds(zz * 256 + (peer // 4) * 128, 128)].astype(F32)
                shift = ((k - peer % 4) * OWN) % 128
                if shift:
                    src = pltpu.roll(src, shift, 1)
                tile = src if tile is None else jnp.where(lane_block == k, src, tile)
            lanes = pl.ds(half * 128, 128)
            sq_send[peer, :, lanes] = jnp.sum(tile * tile, axis=0, keepdims=True)
            x_send[peer, :, lanes] = (tile * gain_col).astype(BF16)

    pl.semaphore_wait(barrier, len(peers + z_near))

    def relay_out(k):
        for peer in z_near:
            pl.semaphore_signal(relay_sem.at[k], inc=1, device_id=peer, device_id_type=MESH_ID)

    def relay_in(k):
        pl.semaphore_wait(relay_sem.at[k], 2)

    relay_out(0)

    kinds, arrivals = {}, {}

    def go(src, dst, kind, arrival, peer):
        copy = pltpu.make_async_remote_copy(
            src_ref=src,
            dst_ref=dst,
            send_sem=send_sems.at[kinds.setdefault(kind, len(kinds))],
            recv_sem=recv_sems.at[arrivals.setdefault((kind, arrival), len(arrivals))],
            device_id=peer,
            device_id_type=MESH_ID,
        )
        copy.start()
        return copy

    def await_bytes(ref, kind, arrival):
        sem = recv_sems.at[arrivals[kind, arrival]]
        pltpu.make_async_copy(ref, ref, sem).wait()

    for dy in (2, 1, 3):
        py = at_y(dy)
        src = x_send.at[pl.ds(py * C, C)]
        go(src, x_all.at[SLOT[dy]], "x", dy, (z, py, c, x))
    x_all[0] = x_send[pl.ds(y * C, C)]

    for i, (dy, dc) in enumerate(group_steps):
        py, pc = group_peer(dy, dc)
        go(sq_send.at[py * C + pc], sq_all.at[i], "sq", 0, (z, py, pc, x))

    for j, (start, width) in enumerate(CHUNKS):
        for copy in w_loads[j]:
            copy.wait()
        cols = pl.ds(start, width)
        for dy in (2, 1, 3):
            dst = w_all.at[SLOT[dy], :, cols]
            go(w_all.at[0, :, cols], dst, "w", j, (z, at_y(dy), c, x))
    w_loads[-1][0].wait()
    for dy in (2, 1, 3):
        go(wo_all.at[0], wo_all.at[SLOT[dy] * C], "wo", 0, (z, at_y(dy), c, x))
    go(wo_all.at[0], wo_all.at[1], "wo", 1, (z, y, sib, x))

    def out_weights_across():
        await_bytes(wo_all.at[pl.ds(0, Y - 1)], "wo", 0)
        for k in range(1, Y):
            go(wo_all.at[k * C], wo_all.at[k * C + 1], "wo", 1, (z, y, sib, x))

    def out_weights_in():
        await_bytes(wo_all.at[pl.ds(0, Y)], "wo", 1)

    for copy in base_loads:
        copy.wait()
    position = lax.broadcasted_iota(jnp.int32, (STEPS, COLS), 0)
    decays, keys_old, values_old = [], [], []
    for s in range(SEQS):
        taken = position < accepted_ref[s]
        gate = jnp.where(taken, prev_gate_ref[s], 1.0)
        key = 1.0 - gate
        after = jnp.ones((1, COLS), F32)
        rows = [None] * STEPS
        for j in reversed(range(STEPS)):
            rows[j] = key[j : j + 1] * after
            after = after * gate[j : j + 1]
        decays.append(after)
        keys_old.append(jnp.concatenate(rows, axis=0))
        values_old.append(prev_value_ref[s].astype(F32))
    for h in range(HEADS):
        cols = slice(h * HEAD, (h + 1) * HEAD)
        decay_cols = jnp.transpose(
            jnp.concatenate([decays[s][:, cols] for s in range(SEQS)], axis=0)
        )
        for s in range(SEQS):
            added = lax.dot_general(
                keys_old[s][:, cols],
                values_old[s][:, cols],
                (((0,), (0,)), ((), ())),
                precision=lax.Precision.HIGHEST,
                preferred_element_type=F32,
            )
            new = base_ref[s, h] * decay_cols[:, s : s + 1] + added
            base_ref[s, h] = new
            base_low[s, h] = new.astype(BF16)

    def squares_out():
        await_bytes(sq_all, "sq", 0)
        total = sq_send[g]
        for k in range(G - 1):
            total = total + sq_all[k]
        sq_mine[...] = total
        for dz in range(1, Z):
            go(sq_mine, sq_z.at[z], "sqz", 0, (at_z(dz), y, c, x))
        sq_z[z] = total

    def token_scale():
        await_bytes(sq_z.at[pl.ds(0, Z - 1)], "sqz", 0)
        squares = sq_z[0]
        for k in range(1, Z):
            squares = squares + sq_z[k]
        token = lax.broadcasted_iota(jnp.int32, (OWN, SET), 0) + z * OWN
        lane = lax.broadcasted_iota(jnp.int32, (OWN, SET), 1)
        own_squares = jnp.sum(
            jnp.where(lane == token, jnp.broadcast_to(squares, (OWN, SET)), 0.0),
            axis=1,
            keepdims=True,
        )
        return lax.rsqrt(own_squares / D + EPSILON)

    def inputs_in(pair):
        for dy in ((1,), (3, 2))[pair]:
            await_bytes(x_all.at[SLOT[dy]], "x", dy)
        for k in range(C):
            block = jnp.concatenate((x_all[2 * pair, k], x_all[2 * pair + 1, k]), axis=0)
            left_ref[k, :, pl.ds(pair * HEAD, HEAD)] = jnp.transpose(block)

    def multiply(j):
        start, width = CHUNKS[j]
        cols = pl.ds(start, width)
        await_bytes(w_all.at[pl.ds(1, Y - 1), :, cols], "w", j)
        right = w_all[:, :, cols].reshape(Y * FEATS, width)
        other = jnp.dot(left_ref[sib], right, preferred_element_type=F32)
        half_send[:, :, cols] = other.astype(BF16).reshape(Z, OWN, width)
        go(half_send.at[:, :, cols], half_recv.at[:, :, cols], "half", j, (z, y, sib, x))
        own = jnp.dot(left_ref[c], right, preferred_element_type=F32)
        part[:, :, cols] = own.reshape(Z, OWN, width)

    def to_neighbour(j, way, m, value, to):
        cols = pl.ds(*CHUNKS[j])
        first_send[way * 2 + m, :, cols] = value.astype(BF16)
        src, dst = first_send.at[way * 2 + m, :, cols], first_recv.at[way * 2 + m, :, cols]
        go(src, dst, "first", (j, way, m), (to, y, c, x))

    def to_owner(j, way, m, value, to):
        cols = pl.ds(*CHUNKS[j])
        second_send[way * 2 + m, :, cols] = value.astype(BF16)
        src, dst = second_send.at[way * 2 + m, :, cols], second_recv.at[way * 2 + m, :, cols]
        go(src, dst, "second", j, (to, y, c, x))

    WAYS = ((UP, 1), (DOWN, -1))

    def distribute(j):
        cols = pl.ds(*CHUNKS[j])
        await_bytes(half_recv.at[:, :, cols], "half", j)
        part[:, :, cols] = part[:, :, cols] + half_recv[:, :, cols].astype(F32)
        for way, sign in WAYS:
            for m, (far, near) in enumerate(MERGES[HOPS[j][way]]):
                if far is None:
                    to_owner(j, way, m, part[at_z(sign * near), :, cols], at_z(sign * near))
                else:
                    to_neighbour(j, way, m, part[at_z(sign * far), :, cols], at_z(sign))

    def merge(j):
        cols = pl.ds(*CHUNKS[j])
        for m in range(2):
            for way, sign in WAYS:
                far, near = MERGES[HOPS[j][way]][m]
                if far is not None:
                    await_bytes(first_recv.at[way * 2 + m, :, cols], "first", (j, way, m))
                    value = part[at_z(sign * near), :, cols]
                    value = value + first_recv[way * 2 + m, :, cols].astype(F32)
                    to_owner(j, way, m, value, at_z(sign * near))

    row = lax.broadcasted_iota(jnp.int32, (OWN, HEAD), 0)
    when = lax.rem(row, STEPS)
    first_seq = lax.broadcasted_iota(jnp.int32, (8, HEAD), 0) < STEPS
    def recur(h, rscale):
        cols = pl.ds(*CHUNKS[h])
        await_bytes(second_recv.at[:, :, cols], "second", h)
        total = part[z, :, cols]
        for k in range(4):
            total = total + second_recv[k, :, cols].astype(F32)
        total = total * rscale
        floor = floor_ref[h : h + 1, :]
        gate = floor + (1.0 - floor) * jax.nn.sigmoid(total[:, HEAD : 2 * HEAD])
        key = 1.0 - gate
        pre = total[:, :HEAD]
        query = pre * jax.nn.sigmoid(pre)
        value = total[:, 2 * HEAD :]
        decayed = query
        result = jnp.sum(query * key, axis=1, keepdims=True) * value
        for back in range(1, STEPS):
            gate_back = gate if back == 1 else pltpu.roll(gate, back - 1, 0)
            decayed = decayed * (
                gate_back if back == 1 else jnp.where(when >= back - 1, gate_back, 1.0)
            )
            weight = jnp.sum(
                jnp.where(when >= back, decayed * pltpu.roll(key, back, 0), 0.0),
                axis=1,
                keepdims=True,
            )
            result = result + weight * pltpu.roll(value, back, 0)
        decayed = decayed * jnp.where(when >= STEPS - 1, pltpu.roll(gate, STEPS - 1, 0), 1.0)
        low = decayed.astype(BF16)
        carried = []
        for pair in range(SEQS // 2):
            rows = low[pair * 8 : pair * 8 + 8]
            one = jnp.dot(rows, base_low[2 * pair, h], preferred_element_type=F32)
            two = jnp.dot(rows, base_low[2 * pair + 1, h], preferred_element_type=F32)
            carried.append(jnp.where(first_seq, one, two))
        result = result + jnp.concatenate(carried, axis=0)
        mean = jnp.sum(result * result, axis=1, keepdims=True) / HEAD
        normed = result * lax.rsqrt(mean + EPSILON) * head_gain_ref[h : h + 1, :]
        normed_all[z, h] = normed.astype(BF16)
        slot = normed_all.at[z, h]
        for dz in (4, 3, 5, 2, 6, 1, 7):
            go(slot, slot, "normed", h, (at_z(dz), y, c, x))

    relay_in(0)
    relay_out(1)
    inputs_in(0)
    relay_in(1)
    relay_out(2)
    inputs_in(1)
    multiply(0)
    distribute(0)
    multiply(1)
    distribute(1)
    multiply(2)
    merge(0)
    distribute(2)
    relay_in(2)
    squares_out()
    multiply(3)
    distribute(3)
    merge(1)
    merge(2)
    merge(3)
    for copy in small_loads:
        copy.wait()
    rscale = token_scale()
    recur(0, rscale)
    recur(1, rscale)
    out_weights_across()
    recur(2, rscale)
    recur(3, rscale)
    out_weights_in()

    product = None
    for h in range(HEADS):
        await_bytes(normed_all.at[pl.ds(0, Z - 1), h], "normed", h)
        term = lax.dot_general(
            wo_all[:, :, pl.ds(h * HEAD, HEAD)].reshape(G * FEATS, HEAD),
            normed_all[:, h].reshape(SET, HEAD),
            (((1,), (1,)), ((), ())),
            preferred_element_type=F32,
        )
        product = term if product is None else product + term
    final_send[...] = product.astype(BF16).reshape(Y, C, X, FEATS // X, SET)
    final_recv[x * G + g] = final_send[0, 0, x]
    for dy, dx, dc in [(dy, dx, dc) for dy in (2, 1, 3, 0) for dx in (2, 1, 3, 0) for dc in (0, 1)]:
        if dy or dx or dc:
            peer = (z, at_y(-dy), sib if dc else c, at_x(dx))
            src, dst = final_send.at[SLOT[dy], dc, peer[3]], final_recv.at[x * G + g]
            go(src, dst, "final", 0, peer)
    await_bytes(final_recv.at[pl.ds(0, X * G - 1)], "final", 0)

    rows_out = FEATS // X
    for k in range(G):
        total = final_recv[k].astype(F32)
        for m in range(1, X):
            total = total + final_recv[m * G + k].astype(F32)
        out_ref[k] = total.astype(BF16)

    sent = {
        "x": x_all.at[pl.ds(1, Y - 1)],
        "w": w_all.at[pl.ds(1, Y - 1)],
        "sq": sq_all,
        "wo": wo_all.at[pl.ds(0, G - 1)],
        "sqz": sq_z.at[pl.ds(0, Z - 1)],
        "half": half_recv,
        "first": first_recv.at[pl.ds(0, 3)],
        "second": second_recv,
        "normed": normed_all.at[pl.ds(0, Z - 1)],
        "final": final_recv.at[pl.ds(0, X * G - 1)],
    }
    for kind, ref in sent.items():
        pltpu.make_async_copy(ref, ref, send_sems.at[kinds[kind]]).wait()
    assert len(kinds) == KINDS and len(arrivals) == ARRIVALS


def tail(pieces_ref, base_ref, out_ref, base_hbm, sems):
    stores = []
    for s in range(SEQS):
        store = pltpu.make_async_copy(base_ref.at[s], base_hbm.at[s], sems.at[s])
        store.start()
        stores.append(store)
    rows_out = FEATS // X
    lane_block = lax.broadcasted_iota(jnp.int32, (rows_out, HEAD), 1) // OWN
    for zz in range(Z):
        for half_g in range(2):
            tile = None
            for k in range(4):
                src = pieces_ref[half_g * 4 + k, :, pl.ds((zz // 4) * 128, 128)].astype(F32)
                shift = ((k - zz % 4) * OWN) % 128
                if shift:
                    src = pltpu.roll(src, shift, 1)
                tile = src if tile is None else jnp.where(lane_block == k, src, tile)
            out_ref[:, pl.ds(zz * 256 + half_g * 128, 128)] = tile.astype(BF16)
    for store in stores:
        store.wait()


def fused(*args):
    any_space = pl.BlockSpec(memory_space=pl.ANY)
    vmem = pl.BlockSpec(memory_space=pltpu.VMEM)
    pieces, base = pl.pallas_call(
        kernel,
        out_shape=(
            pltpu.VMEM((G, FEATS // X, SET), BF16),
            pltpu.VMEM((SEQS, HEADS, HEAD, HEAD), F32),
        ),
        in_specs=[any_space] * 12,
        out_specs=(vmem, vmem),
        scratch_shapes=[
            pltpu.VMEM((1, FEATS), BF16),
            pltpu.VMEM((HEADS, HEAD), F32),
            pltpu.VMEM((HEADS, HEAD), F32),
            pltpu.VMEM((SEQS, STEPS, COLS), F32),
            pltpu.VMEM((SEQS, STEPS, COLS), BF16),
            pltpu.SMEM((SEQS,), jnp.int32),
            pltpu.VMEM((FEATS, TOKENS), BF16),
            pltpu.VMEM((G, FEATS, SET), BF16),
            pltpu.VMEM((Y, C, FEATS, SET), BF16),
            pltpu.VMEM((C, SET, Y * FEATS), BF16),
            pltpu.VMEM((Z, OWN, HEADS * WIDE), BF16),
            pltpu.VMEM((Z, OWN, HEADS * WIDE), BF16),
            pltpu.VMEM((G, 1, SET), F32),
            pltpu.VMEM((G - 1, 1, SET), F32),
            pltpu.VMEM((1, SET), F32),
            pltpu.VMEM((Z, 1, SET), F32),
            pltpu.VMEM((Y, FEATS, HEADS * WIDE), BF16),
            pltpu.VMEM((G, FEATS, COLS), BF16),
            pltpu.VMEM((SEQS, HEADS, HEAD, HEAD), BF16),
            pltpu.VMEM((Z, OWN, HEADS * WIDE), F32),
            pltpu.VMEM((4, OWN, HEADS * WIDE), BF16),
            pltpu.VMEM((4, OWN, HEADS * WIDE), BF16),
            pltpu.VMEM((4, OWN, HEADS * WIDE), BF16),
            pltpu.VMEM((4, OWN, HEADS * WIDE), BF16),
            pltpu.VMEM((Z, HEADS, OWN, HEAD), BF16),
            pltpu.VMEM((Y, C, X, FEATS // X, SET), BF16),
            pltpu.VMEM((X * G, FEATS // X, SET), BF16),
            pltpu.SemaphoreType.REGULAR((3,)),
            pltpu.SemaphoreType.DMA((13,)),
            pltpu.SemaphoreType.DMA((KINDS,)),
            pltpu.SemaphoreType.DMA((ARRIVALS,)),
        ],
        compiler_params=pltpu.CompilerParams(collective_id=0, has_side_effects=True),
    )(*args)
    return pl.pallas_call(
        tail,
        out_shape=(
            jax.ShapeDtypeStruct((FEATS // X, TOKENS), BF16),
            jax.ShapeDtypeStruct((SEQS, HEADS, HEAD, HEAD), F32),
        ),
        in_specs=[vmem, vmem],
        out_specs=(vmem, any_space),
        scratch_shapes=[pltpu.SemaphoreType.DMA((SEQS,))],
        compiler_params=pltpu.CompilerParams(vmem_limit_bytes=8 * 2**20),
    )(pieces, base)


def body(
    inputs,
    norm_gain,
    w_query,
    w_forget,
    w_value,
    lower_bound,
    head_gain,
    w_out,
    prior_state,
    prev_forget,
    prev_values,
    accepted,
):
    mixed, base_state = fused(
        inputs.T,
        norm_gain.reshape(1, FEATS),
        w_query,
        w_forget,
        w_value,
        w_out.T,
        lower_bound.reshape(HEADS, HEAD),
        head_gain.reshape(HEADS, HEAD),
        prior_state,
        prev_forget,
        prev_values,
        accepted,
    )
    return (mixed.T, base_state)


def solution(mesh):
    split = Mesh(mesh.devices.reshape(Z, Y, C, X), KV_TP)
    placed = (
        P(None, KV),
        P(KV),
        P(KV, "tp"),
        P(KV, "tp"),
        P(KV, "tp"),
        P("tp"),
        P("tp"),
        P("tp", KV),
        P(KV, "tp", None, None),
        P(KV, None, "tp"),
        P(KV, None, "tp"),
        P(KV),
    )
    return jax.shard_map(
        body,
        mesh=split,
        in_specs=placed,
        out_specs=(P(None, KV_TP), P(KV, "tp", None, None)),
        check_vma=False,
    )
```

```python
import functools

import jax
import jax.numpy as jnp
from jax import lax
from jax.experimental import pallas as pl
from jax.experimental.pallas import tpu as pltpu
from jax.sharding import Mesh
from jax.sharding import PartitionSpec as P

KV = ("kv_0", "kv_1", "kv_2")
KV_TP = ("kv_0", "kv_1", "kv_2", "tp")
MESH_ID = pl.DeviceIdType.MESH
EPSILON = 1e-06
F32 = jnp.float32
BF16 = jnp.bfloat16

D = 4096
Z, Y, C, X = 8, 4, 2, 4
G = Y * C
FEATS = 64
OWN = 32
SET = Z * OWN
TOKENS = 2048
HEADS = 4
HEAD = 128
COLS = HEADS * HEAD
SEQS = 8
STEPS = 4
UP, DOWN = 0, 1
WIDE = 3 * HEAD
CHUNKS = ((0, 384), (384, 384), (768, 384), (1152, 384))
HOPS = ((4, 3), (3, 4), (4, 3), (3, 4))
SLOT = (0, 1, 3, 2)
MERGES = {4: ((4, 3), (2, 1)), 3: ((3, 2), (None, 1))}
KINDS = 11
ARRIVALS = 35


def kernel(
    x_hbm,
    gain_hbm,
    wq_hbm,
    wf_hbm,
    wv_hbm,
    wo_hbm,
    floor_hbm,
    head_gain_hbm,
    prior_hbm,
    prev_gate_hbm,
    prev_value_hbm,
    accepted_hbm,
    out_ref,
    base_ref,
    gain_ref,
    floor_ref,
    head_gain_ref,
    prev_gate_ref,
    prev_value_ref,
    accepted_ref,
    x_raw,
    x_send,
    x_all,
    left_ref,
    half_send,
    half_recv,
    sq_send,
    sq_all,
    sq_mine,
    sq_z,
    w_all,
    wo_all,
    base_low,
    part,
    first_send,
    first_recv,
    second_send,
    second_recv,
    normed_all,
    final_send,
    final_recv,
    relay_sem,
    local_sem,
    send_sems,
    recv_sems,
):
    z = lax.axis_index("kv_0")
    y = lax.axis_index("kv_1")
    c = lax.axis_index("kv_2")
    x = lax.axis_index("tp")
    g = y * C + c

    def at_z(step):
        return lax.rem(z + (step + Z), Z)

    def at_y(step):
        return lax.rem(y + (step + Y), Y)

    def at_x(step):
        return lax.rem(x + (step + X), X)

    sib = 1 - c
    group_steps = [(2, 0), (2, 1), (1, 0), (1, 1), (3, 0), (3, 1), (0, 1)]

    def group_peer(dy, dc):
        return at_y(dy), (sib if dc else c)

    barrier = pltpu.get_barrier_semaphore()
    z_near = [(at_z(1), y, c, x), (at_z(-1), y, c, x)]
    peers = []
    for dy, dc in group_steps:
        py, pc = group_peer(dy, dc)
        peers.append((z, py, pc, x))
    for dx in (2, 1, 3):
        peers.append((z, y, c, at_x(dx)))
    for peer in peers + z_near:
        pl.semaphore_signal(barrier, inc=1, device_id=peer, device_id_type=MESH_ID)

    def load(src, dst, index):
        copy = pltpu.make_async_copy(src, dst, local_sem.at[index])
        copy.start()
        return copy

    def load_weights(j):
        start, width = CHUNKS[j]
        for k in range(start // HEAD, (start + width) // HEAD):
            src = (wq_hbm, wf_hbm, wv_hbm)[k % 3].at[:, pl.ds(k // 3 * HEAD, HEAD)]
            load(src, w_all.at[0, :, pl.ds(k * HEAD, HEAD)], j)
        own = w_all.at[0, :, pl.ds(start, width)]
        return [pltpu.make_async_copy(own, own, local_sem.at[j])]

    w_loads = [load_weights(0)]
    x_load = load(x_hbm, x_raw, 4)
    gain_load = load(gain_hbm, gain_ref, 5)
    w_loads += [load_weights(j) for j in range(1, len(CHUNKS))]
    base_loads = [
        load(prior_hbm, base_ref, 6),
        load(prev_gate_hbm, prev_gate_ref, 7),
        load(prev_value_hbm, prev_value_ref, 8),
        load(accepted_hbm, accepted_ref, 9),
    ]
    small_loads = [load(floor_hbm, floor_ref, 10), load(head_gain_hbm, head_gain_ref, 11)]
    w_loads.append([load(wo_hbm, wo_all.at[0], 12)])

    x_load.wait()
    gain_load.wait()
    gain_col = jnp.transpose(jnp.broadcast_to(gain_ref[...].astype(F32), (HEAD, FEATS)))
    lane_block = lax.broadcasted_iota(jnp.int32, (FEATS, HEAD), 1) // OWN
    for peer in range(G):
        for half in range(2):
            tile = None
            for k in range(4):
                zz = half * 4 + k
                src = x_raw[:, pl.ds(zz * 256 + (peer // 4) * 128, 128)].astype(F32)
                shift = ((k - peer % 4) * OWN) % 128
                if shift:
                    src = pltpu.roll(src, shift, 1)
                tile = src if tile is None else jnp.where(lane_block == k, src, tile)
            lanes = pl.ds(half * 128, 128)
            sq_send[peer, :, lanes] = jnp.sum(tile * tile, axis=0, keepdims=True)
            x_send[peer, :, lanes] = (tile * gain_col).astype(BF16)

    pl.semaphore_wait(barrier, len(peers + z_near))

    def relay_out(k):
        for peer in z_near:
            pl.semaphore_signal(relay_sem.at[k], inc=1, device_id=peer, device_id_type=MESH_ID)

    def relay_in(k):
        pl.semaphore_wait(relay_sem.at[k], 2)

    relay_out(0)

    kinds, arrivals = {}, {}

    def go(src, dst, kind, arrival, peer):
        copy = pltpu.make_async_remote_copy(
            src_ref=src,
            dst_ref=dst,
            send_sem=send_sems.at[kinds.setdefault(kind, len(kinds))],
            recv_sem=recv_sems.at[arrivals.setdefault((kind, arrival), len(arrivals))],
            device_id=peer,
            device_id_type=MESH_ID,
        )
        copy.start()
        return copy

    def await_bytes(ref, kind, arrival):
        sem = recv_sems.at[arrivals[kind, arrival]]
        pltpu.make_async_copy(ref, ref, sem).wait()

    quarter = FEATS // X
    mine = pl.ds(pl.multiple_of(x * quarter, quarter), quarter)
    for dy in (1, 3, 2):
        py = at_y(dy)
        src = x_send.at[pl.ds(py * C, C), mine]
        go(src, x_all.at[SLOT[dy], :, mine], "x", 0, (z, py, c, x))
    x_all[0] = x_send[pl.ds(y * C, C)]

    for i, (dy, dc) in enumerate(group_steps):
        py, pc = group_peer(dy, dc)
        go(sq_send.at[py * C + pc], sq_all.at[i], "sq", 0, (z, py, pc, x))

    for j, (start, width) in enumerate(CHUNKS):
        for copy in w_loads[j]:
            copy.wait()
        cols = pl.ds(start, width)
        for dy in (1, 3, 2):
            dst = w_all.at[SLOT[dy], :, cols]
            go(w_all.at[0, :, cols], dst, "w", j, (z, at_y(dy), c, x))
    w_loads[-1][0].wait()
    for dy in (2, 1, 3):
        go(wo_all.at[0], wo_all.at[SLOT[dy] * C], "wo", 0, (z, at_y(dy), c, x))
    go(wo_all.at[0], wo_all.at[1], "wo", 1, (z, y, sib, x))

    def out_weights_across():
        await_bytes(wo_all.at[pl.ds(0, Y - 1)], "wo", 0)
        for k in range(1, Y):
            go(wo_all.at[k * C], wo_all.at[k * C + 1], "wo", 1, (z, y, sib, x))

    def out_weights_in():
        await_bytes(wo_all.at[pl.ds(0, Y)], "wo", 1)

    for copy in base_loads:
        copy.wait()
    position = lax.broadcasted_iota(jnp.int32, (STEPS, COLS), 0)
    decays, keys_old, values_old = [], [], []
    for s in range(SEQS):
        taken = position < accepted_ref[s]
        gate = jnp.where(taken, prev_gate_ref[s], 1.0)
        key = 1.0 - gate
        after = jnp.ones((1, COLS), F32)
        rows = [None] * STEPS
        for j in reversed(range(STEPS)):
            rows[j] = key[j : j + 1] * after
            after = after * gate[j : j + 1]
        decays.append(after)
        keys_old.append(jnp.concatenate(rows, axis=0))
        values_old.append(prev_value_ref[s].astype(F32))
    for h in range(HEADS):
        cols = slice(h * HEAD, (h + 1) * HEAD)
        decay_cols = jnp.transpose(
            jnp.concatenate([decays[s][:, cols] for s in range(SEQS)], axis=0)
        )
        for s in range(SEQS):
            added = lax.dot_general(
                keys_old[s][:, cols],
                values_old[s][:, cols],
                (((0,), (0,)), ((), ())),
                precision=lax.Precision.HIGHEST,
                preferred_element_type=F32,
            )
            new = base_ref[s, h] * decay_cols[:, s : s + 1] + added
            base_ref[s, h] = new
            base_low[s, h] = new.astype(BF16)

    def squares_out():
        await_bytes(sq_all, "sq", 0)
        total = sq_send[g]
        for k in range(G - 1):
            total = total + sq_all[k]
        sq_mine[...] = total
        for dz in range(1, Z):
            go(sq_mine, sq_z.at[z], "sqz", 0, (at_z(dz), y, c, x))
        sq_z[z] = total

    def token_scale():
        await_bytes(sq_z.at[pl.ds(0, Z - 1)], "sqz", 0)
        squares = sq_z[0]
        for k in range(1, Z):
            squares = squares + sq_z[k]
        token = lax.broadcasted_iota(jnp.int32, (OWN, SET), 0) + z * OWN
        lane = lax.broadcasted_iota(jnp.int32, (OWN, SET), 1)
        own_squares = jnp.sum(
            jnp.where(lane == token, jnp.broadcast_to(squares, (OWN, SET)), 0.0),
            axis=1,
            keepdims=True,
        )
        return lax.rsqrt(own_squares / D + EPSILON)

    def inputs_across():
        rows = x_all.at[pl.ds(1, Y - 1), :, mine]
        await_bytes(rows, "x", 0)
        for dx in (1, 3, 2):
            go(rows, rows, "x across", 0, (z, y, c, at_x(dx)))

    def inputs_in():
        others = x_all.at[pl.ds(1, Y - 1), :, pl.ds(0, FEATS - quarter)]
        await_bytes(others, "x across", 0)
        for pair in range(Y // 2):
            for k in range(C):
                block = jnp.concatenate((x_all[2 * pair, k], x_all[2 * pair + 1, k]), axis=0)
                left_ref[k, :, pl.ds(pair * HEAD, HEAD)] = jnp.transpose(block)

    def multiply(j):
        start, width = CHUNKS[j]
        cols = pl.ds(start, width)
        await_bytes(w_all.at[pl.ds(1, Y - 1), :, cols], "w", j)
        right = w_all[:, :, cols].reshape(Y * FEATS, width)
        other = jnp.dot(left_ref[sib], right, preferred_element_type=F32)
        half_send[:, :, cols] = other.astype(BF16).reshape(Z, OWN, width)
        go(half_send.at[:, :, cols], half_recv.at[:, :, cols], "half", j, (z, y, sib, x))
        own = jnp.dot(left_ref[c], right, preferred_element_type=F32)
        part[:, :, cols] = own.reshape(Z, OWN, width)

    def to_neighbour(j, way, m, value, to):
        cols = pl.ds(*CHUNKS[j])
        first_send[way * 2 + m, :, cols] = value.astype(BF16)
        src, dst = first_send.at[way * 2 + m, :, cols], first_recv.at[way * 2 + m, :, cols]
        go(src, dst, "first", (j, way, m), (to, y, c, x))

    def to_owner(j, way, m, value, to):
        cols = pl.ds(*CHUNKS[j])
        second_send[way * 2 + m, :, cols] = value.astype(BF16)
        src, dst = second_send.at[way * 2 + m, :, cols], second_recv.at[way * 2 + m, :, cols]
        go(src, dst, "second", j, (to, y, c, x))

    WAYS = ((UP, 1), (DOWN, -1))

    def distribute(j):
        cols = pl.ds(*CHUNKS[j])
        await_bytes(half_recv.at[:, :, cols], "half", j)
        part[:, :, cols] = part[:, :, cols] + half_recv[:, :, cols].astype(F32)
        for way, sign in WAYS:
            for m, (far, near) in enumerate(MERGES[HOPS[j][way]]):
                if far is None:
                    to_owner(j, way, m, part[at_z(sign * near), :, cols], at_z(sign * near))
                else:
                    to_neighbour(j, way, m, part[at_z(sign * far), :, cols], at_z(sign))

    def merge(j):
        cols = pl.ds(*CHUNKS[j])
        for m in range(2):
            for way, sign in WAYS:
                far, near = MERGES[HOPS[j][way]][m]
                if far is not None:
                    await_bytes(first_recv.at[way * 2 + m, :, cols], "first", (j, way, m))
                    value = part[at_z(sign * near), :, cols]
                    value = value + first_recv[way * 2 + m, :, cols].astype(F32)
                    to_owner(j, way, m, value, at_z(sign * near))

    row = lax.broadcasted_iota(jnp.int32, (OWN, HEAD), 0)
    when = lax.rem(row, STEPS)
    first_seq = lax.broadcasted_iota(jnp.int32, (8, HEAD), 0) < STEPS
    def recur(h, rscale):
        cols = pl.ds(*CHUNKS[h])
        await_bytes(second_recv.at[:, :, cols], "second", h)
        total = part[z, :, cols]
        for k in range(4):
            total = total + second_recv[k, :, cols].astype(F32)
        total = total * rscale
        floor = floor_ref[h : h + 1, :]
        gate = floor + (1.0 - floor) * jax.nn.sigmoid(total[:, HEAD : 2 * HEAD])
        key = 1.0 - gate
        pre = total[:, :HEAD]
        query = pre * jax.nn.sigmoid(pre)
        value = total[:, 2 * HEAD :]
        decayed = query
        result = jnp.sum(query * key, axis=1, keepdims=True) * value
        for back in range(1, STEPS):
            gate_back = gate if back == 1 else pltpu.roll(gate, back - 1, 0)
            decayed = decayed * (
                gate_back if back == 1 else jnp.where(when >= back - 1, gate_back, 1.0)
            )
            weight = jnp.sum(
                jnp.where(when >= back, decayed * pltpu.roll(key, back, 0), 0.0),
                axis=1,
                keepdims=True,
            )
            result = result + weight * pltpu.roll(value, back, 0)
        decayed = decayed * jnp.where(when >= STEPS - 1, pltpu.roll(gate, STEPS - 1, 0), 1.0)
        low = decayed.astype(BF16)
        carried = []
        for pair in range(SEQS // 2):
            rows = low[pair * 8 : pair * 8 + 8]
            one = jnp.dot(rows, base_low[2 * pair, h], preferred_element_type=F32)
            two = jnp.dot(rows, base_low[2 * pair + 1, h], preferred_element_type=F32)
            carried.append(jnp.where(first_seq, one, two))
        result = result + jnp.concatenate(carried, axis=0)
        mean = jnp.sum(result * result, axis=1, keepdims=True) / HEAD
        normed = result * lax.rsqrt(mean + EPSILON) * head_gain_ref[h : h + 1, :]
        normed_all[z, h] = normed.astype(BF16)
        slot = normed_all.at[z, h]
        for dz in (4, 3, 5, 2, 6, 1, 7):
            go(slot, slot, "normed", h, (at_z(dz), y, c, x))

    relay_in(0)
    relay_out(1)
    inputs_across()
    relay_in(1)
    relay_out(2)
    inputs_in()
    multiply(0)
    distribute(0)
    multiply(1)
    distribute(1)
    multiply(2)
    merge(0)
    distribute(2)
    relay_in(2)
    squares_out()
    multiply(3)
    distribute(3)
    merge(1)
    merge(2)
    merge(3)
    for copy in small_loads:
        copy.wait()
    rscale = token_scale()
    recur(0, rscale)
    recur(1, rscale)
    out_weights_across()
    recur(2, rscale)
    recur(3, rscale)
    out_weights_in()

    product = None
    for h in range(HEADS):
        await_bytes(normed_all.at[pl.ds(0, Z - 1), h], "normed", h)
        term = lax.dot_general(
            wo_all[:, :, pl.ds(h * HEAD, HEAD)].reshape(G * FEATS, HEAD),
            normed_all[:, h].reshape(SET, HEAD),
            (((1,), (1,)), ((), ())),
            preferred_element_type=F32,
        )
        product = term if product is None else product + term
    final_send[...] = product.astype(BF16).reshape(Y, C, X, FEATS // X, SET)
    final_recv[x * G + g] = final_send[0, 0, x]
    for dy, dx, dc in [(dy, dx, dc) for dy in (2, 1, 3, 0) for dx in (2, 1, 3, 0) for dc in (0, 1)]:
        if dy or dx or dc:
            peer = (z, at_y(-dy), sib if dc else c, at_x(dx))
            src, dst = final_send.at[SLOT[dy], dc, peer[3]], final_recv.at[x * G + g]
            go(src, dst, "final", 0, peer)
    await_bytes(final_recv.at[pl.ds(0, X * G - 1)], "final", 0)

    rows_out = FEATS // X
    for k in range(G):
        total = final_recv[k].astype(F32)
        for m in range(1, X):
            total = total + final_recv[m * G + k].astype(F32)
        out_ref[k] = total.astype(BF16)

    sent = {
        "x": x_all.at[pl.ds(1, Y - 1), :, pl.ds(0, quarter)],
        "x across": x_all.at[pl.ds(1, Y - 1), :, pl.ds(0, FEATS - quarter)],
        "w": w_all.at[pl.ds(1, Y - 1)],
        "sq": sq_all,
        "wo": wo_all.at[pl.ds(0, G - 1)],
        "sqz": sq_z.at[pl.ds(0, Z - 1)],
        "half": half_recv,
        "first": first_recv.at[pl.ds(0, 3)],
        "second": second_recv,
        "normed": normed_all.at[pl.ds(0, Z - 1)],
        "final": final_recv.at[pl.ds(0, X * G - 1)],
    }
    for kind, ref in sent.items():
        pltpu.make_async_copy(ref, ref, send_sems.at[kinds[kind]]).wait()
    assert len(kinds) == KINDS and len(arrivals) == ARRIVALS


def tail(pieces_ref, base_ref, out_ref, base_hbm, sems):
    stores = []
    for s in range(SEQS):
        store = pltpu.make_async_copy(base_ref.at[s], base_hbm.at[s], sems.at[s])
        store.start()
        stores.append(store)
    rows_out = FEATS // X
    lane_block = lax.broadcasted_iota(jnp.int32, (rows_out, HEAD), 1) // OWN
    for zz in range(Z):
        for half_g in range(2):
            tile = None
            for k in range(4):
                src = pieces_ref[half_g * 4 + k, :, pl.ds((zz // 4) * 128, 128)].astype(F32)
                shift = ((k - zz % 4) * OWN) % 128
                if shift:
                    src = pltpu.roll(src, shift, 1)
                tile = src if tile is None else jnp.where(lane_block == k, src, tile)
            out_ref[:, pl.ds(zz * 256 + half_g * 128, 128)] = tile.astype(BF16)
    for store in stores:
        store.wait()


def fused(*args):
    any_space = pl.BlockSpec(memory_space=pl.ANY)
    vmem = pl.BlockSpec(memory_space=pltpu.VMEM)
    pieces, base = pl.pallas_call(
        kernel,
        out_shape=(
            pltpu.VMEM((G, FEATS // X, SET), BF16),
            pltpu.VMEM((SEQS, HEADS, HEAD, HEAD), F32),
        ),
        in_specs=[any_space] * 12,
        out_specs=(vmem, vmem),
        scratch_shapes=[
            pltpu.VMEM((1, FEATS), BF16),
            pltpu.VMEM((HEADS, HEAD), F32),
            pltpu.VMEM((HEADS, HEAD), F32),
            pltpu.VMEM((SEQS, STEPS, COLS), F32),
            pltpu.VMEM((SEQS, STEPS, COLS), BF16),
            pltpu.SMEM((SEQS,), jnp.int32),
            pltpu.VMEM((FEATS, TOKENS), BF16),
            pltpu.VMEM((G, FEATS, SET), BF16),
            pltpu.VMEM((Y, C, FEATS, SET), BF16),
            pltpu.VMEM((C, SET, Y * FEATS), BF16),
            pltpu.VMEM((Z, OWN, HEADS * WIDE), BF16),
            pltpu.VMEM((Z, OWN, HEADS * WIDE), BF16),
            pltpu.VMEM((G, 1, SET), F32),
            pltpu.VMEM((G - 1, 1, SET), F32),
            pltpu.VMEM((1, SET), F32),
            pltpu.VMEM((Z, 1, SET), F32),
            pltpu.VMEM((Y, FEATS, HEADS * WIDE), BF16),
            pltpu.VMEM((G, FEATS, COLS), BF16),
            pltpu.VMEM((SEQS, HEADS, HEAD, HEAD), BF16),
            pltpu.VMEM((Z, OWN, HEADS * WIDE), F32),
            pltpu.VMEM((4, OWN, HEADS * WIDE), BF16),
            pltpu.VMEM((4, OWN, HEADS * WIDE), BF16),
            pltpu.VMEM((4, OWN, HEADS * WIDE), BF16),
            pltpu.VMEM((4, OWN, HEADS * WIDE), BF16),
            pltpu.VMEM((Z, HEADS, OWN, HEAD), BF16),
            pltpu.VMEM((Y, C, X, FEATS // X, SET), BF16),
            pltpu.VMEM((X * G, FEATS // X, SET), BF16),
            pltpu.SemaphoreType.REGULAR((3,)),
            pltpu.SemaphoreType.DMA((13,)),
            pltpu.SemaphoreType.DMA((KINDS,)),
            pltpu.SemaphoreType.DMA((ARRIVALS,)),
        ],
        compiler_params=pltpu.CompilerParams(collective_id=0, has_side_effects=True),
    )(*args)
    return pl.pallas_call(
        tail,
        out_shape=(
            jax.ShapeDtypeStruct((FEATS // X, TOKENS), BF16),
            jax.ShapeDtypeStruct((SEQS, HEADS, HEAD, HEAD), F32),
        ),
        in_specs=[vmem, vmem],
        out_specs=(vmem, any_space),
        scratch_shapes=[pltpu.SemaphoreType.DMA((SEQS,))],
        compiler_params=pltpu.CompilerParams(vmem_limit_bytes=8 * 2**20),
    )(pieces, base)


def body(
    inputs,
    norm_gain,
    w_query,
    w_forget,
    w_value,
    lower_bound,
    head_gain,
    w_out,
    prior_state,
    prev_forget,
    prev_values,
    accepted,
):
    mixed, base_state = fused(
        inputs.T,
        norm_gain.reshape(1, FEATS),
        w_query,
        w_forget,
        w_value,
        w_out.T,
        lower_bound.reshape(HEADS, HEAD),
        head_gain.reshape(HEADS, HEAD),
        prior_state,
        prev_forget,
        prev_values,
        accepted,
    )
    return (mixed.T, base_state)


def solution(mesh):
    split = Mesh(mesh.devices.reshape(Z, Y, C, X), KV_TP)
    placed = (
        P(None, KV),
        P(KV),
        P(KV, "tp"),
        P(KV, "tp"),
        P(KV, "tp"),
        P("tp"),
        P("tp"),
        P("tp", KV),
        P(KV, "tp", None, None),
        P(KV, None, "tp"),
        P(KV, None, "tp"),
        P(KV),
    )
    return jax.shard_map(
        body,
        mesh=split,
        in_specs=placed,
        out_specs=(P(None, KV_TP), P(KV, "tp", None, None)),
        check_vma=False,
    )
```
